512 devices in a mesh: sp: 64 (over z, y), tp: 8 (over x, core).
Axes of the slice: x: 4, y: 4, z: 16, core: 2. Of those that a mesh axis runs over, the one named last changes fastest.
Arguments:
- query_content: bfloat16 [12288, 1024], P('sp'), may hold values from -6 to 6
- query_rotary: bfloat16 [12288, 512], P('sp'), may hold values from -8 to 8
- latents: bfloat16 [12288, 256], P(('sp', 'tp')), may hold values from -6 to 6
- key_rotary: bfloat16 [12288, 64], P(('sp', 'tp')), may hold values from -8 to 8
- latent_gain: float32 [256], replicated, may hold values from 0.1 to 1.9
- key_up: bfloat16 [256, 1024], P(None, 'tp'), may hold values from -0.375 to 0.375
- value_up: bfloat16 [256, 1024], P(None, 'tp'), may hold values from -0.375 to 0.375
- out_proj: bfloat16 [1024, 2048], P(None, 'tp'), may hold values from -2 to 2
- residual: bfloat16 [12288, 2048], P('sp', 'tp'), may hold values from -6 to 6
- mixer_gain: float32 [2048], replicated, may hold values from 0.1 to 1.9
- gate_proj: bfloat16 [2048, 5632], P('sp', 'tp'), may hold values from -0.125 to 0.125
- up_proj: bfloat16 [2048, 5632], P('sp', 'tp'), may hold values from -0.125 to 0.125
- down_proj: bfloat16 [5632, 2048], P('tp', 'sp'), may hold values from -0.078125 to 0.078125
Outputs:
- layer_out: bfloat16 [12288, 2048], P('sp', 'tp')
The draws below stay inside these ranges and needn't reach their ends.
All inputs are finite; a program needn't handle non-finite values.
Results may differ from the reference program's by a relative error of at most 0.011.
Values may be sent and summed in bfloat16 or wider, within the bound.
No kernel may reach another device: no remote copies, remote signals or barrier semaphores. Data moves between devices by JAX's collectives and lax.ppermute only.
A program may use at most 64 MiB of HBM per device.

```python
import math
import jax
import jax.numpy as jnp
from jax import lax

D = 2048
H = 8
DN = 128
DR = 64
DV = 128
KVR = 256
FF = 5632
SPAN = 64
TOK = 192
SEQ = 12288
N_SP = 64
N_TP = 8


def draw_query_rotary(key, part):
    base = jax.random.normal(jax.random.fold_in(key, 14), (SEQ, H * DR), jnp.float32)
    return jnp.clip(base, -6.0, 6.0).astype(jnp.bfloat16)


def draw_key_rotary(key, part):
    base = jax.random.normal(jax.random.fold_in(key, 15), (SEQ, DR), jnp.float32)
    return jnp.clip(base, -6.0, 6.0).astype(jnp.bfloat16)


def shard_levels(own_key, dims, shards, least, high):
    level, own = 1.0, jax.random.fold_in(own_key, 6)
    for position, parts in shards:
        heights = jnp.exp(jax.random.uniform(jax.random.fold_in(own, position), (parts,), jnp.float32, least / len(shards), high / len(shards)))
        level = level * jnp.repeat(heights, dims[position] // parts).reshape([-1 if axis == position else 1 for axis in range(len(dims))])
    return level


def scatter_about(stream_key, shape, deviation, limit, pieces=(), kind=jnp.bfloat16):
    result = deviation * jax.random.normal(stream_key, shape, jnp.float32)
    if pieces:
        result = result * shard_levels(stream_key, shape, pieces, -0.22, 0.18)
    return jnp.clip(result, -limit, limit).astype(kind)


def setup_inputs(seed: int = 0) -> dict:
    key_of = jax.random.split(jax.random.key(seed), 14)
    query_content = scatter_about(key_of[0], (SEQ, H * DN), 1.0, 6.0, ((0, 64),))
    query_rotary = draw_query_rotary(jax.random.fold_in(key_of[13], 71), 0)
    latents = scatter_about(key_of[2], (SEQ, KVR), 1.0, 6.0, ((0, 512),))
    key_rotary = draw_key_rotary(jax.random.fold_in(key_of[13], 71), 0)
    latent_gain = jnp.clip(1.0 + 0.18 * jax.random.normal(key_of[4], (KVR,), jnp.float32), 0.1, 1.9)
    key_up = scatter_about(key_of[5], (KVR, H * DN), KVR ** -0.5, 0.375, ((1, 8),))
    value_up = scatter_about(key_of[6], (KVR, H * DV), KVR ** -0.5, 0.375, ((1, 8),))
    out_proj = scatter_about(key_of[7], (H * DV, D), (H * DV // 128) ** -0.5, 2.0, ((1, 8),))
    residual = scatter_about(key_of[8], (SEQ, D), 1.0, 6.0, ((0, 64), (1, 8)))
    mixer_gain = jnp.clip(1.0 + 0.18 * jax.random.normal(key_of[9], (D,), jnp.float32), 0.1, 1.9)
    gate_proj = scatter_about(key_of[10], (D, FF), D ** -0.5, 0.125, ((0, 64), (1, 8)))
    up_proj = scatter_about(key_of[11], (D, FF), D ** -0.5, 0.125, ((0, 64), (1, 8)))
    down_proj = scatter_about(key_of[12], (FF, D), FF ** -0.5, 0.078125, ((0, 8), (1, 64)))
    return {"query_content": query_content, "query_rotary": query_rotary, "latents": latents, "key_rotary": key_rotary, "latent_gain": latent_gain, "key_up": key_up, "value_up": value_up, "out_proj": out_proj, "residual": residual, "mixer_gain": mixer_gain, "gate_proj": gate_proj, "up_proj": up_proj, "down_proj": down_proj}


epsilon = 1e-06
masked_score = -1e+30

def norm_round(inputs, scales):
    widened = inputs.astype(jnp.float32)
    factor = lax.rsqrt(lax.optimization_barrier(jnp.mean(widened * widened, axis=-1, keepdims=True)) + epsilon)
    return (widened * factor * scales.astype(jnp.float32)).astype(jnp.bfloat16)

def rotate(inputs, places):
    dimension = inputs.shape[-1]
    middle = dimension // 2
    inverse = 10000.0 ** (-jnp.arange(0, dimension, 2, dtype=jnp.float32) / dimension)
    angles = places.astype(jnp.float32)[:, None, None] * inverse[None, None, :]
    cosine_table = jnp.cos(angles)
    sine_table = jnp.sin(angles)
    widened = inputs.astype(jnp.float32)
    first_half = widened[..., :middle]
    second_half = widened[..., middle:]
    return jnp.concatenate([first_half * cosine_table - second_half * sine_table, second_half * cosine_table + first_half * sine_table], axis=-1).astype(jnp.bfloat16)

def reference(query_content, query_rotary, latents, key_rotary, latent_gain, key_up, value_up, out_proj, residual, mixer_gain, gate_proj, up_proj, down_proj):
    per_device = TOK // N_TP
    normed = norm_round(latents, latent_gain)
    key_content = jnp.dot(normed, key_up, preferred_element_type=jnp.float32).astype(jnp.bfloat16)
    values = jnp.dot(normed, value_up, preferred_element_type=jnp.float32).astype(jnp.bfloat16)
    places = jnp.arange(SEQ, dtype=jnp.int32)
    key_turned = rotate(key_rotary[:, None, :], places)[:, 0, :]
    query_turned = rotate(query_rotary.reshape(SEQ, H, DR), places)
    key_content, values, key_turned, query_turned = lax.optimization_barrier((key_content, values, key_turned, query_turned))

    def subsets(inputs):
        shaped = inputs.reshape((N_SP, N_TP, per_device) + inputs.shape[1:])
        return jnp.swapaxes(shaped, 0, 1).reshape((N_TP, N_SP * per_device) + inputs.shape[1:])
    grouped = (subsets(key_content.reshape(SEQ, H, DN)), subsets(values.reshape(SEQ, H, DV)), subsets(key_turned), subsets(places))
    score_scale = 1.0 / math.sqrt(DN + DR)

    def one_block(query_block):
        contents, turned, query_places = query_block

        def one_subset(subset):
            key_rows, value_rows, key_turns, key_places = subset
            scores = (jnp.einsum('qhd,khd->qhk', contents.astype(jnp.float32), key_rows.astype(jnp.float32)) + jnp.einsum('qhr,kr->qhk', turned.astype(jnp.float32), key_turns.astype(jnp.float32))) * score_scale
            allowed = (key_places[None, :] // SPAN <= query_places[:, None] // SPAN)[:, None, :]
            highest = lax.optimization_barrier(jnp.max(jnp.where(allowed, scores, masked_score), axis=-1))
            weights = jnp.where(allowed, jnp.exp(scores - highest[..., None]), 0.0)
            weight_sum = lax.optimization_barrier(jnp.sum(weights, axis=-1))
            rounded = lax.optimization_barrier(weights.astype(jnp.bfloat16))
            weighted = jnp.einsum('qhk,khv->qhv', rounded.astype(jnp.float32), value_rows.astype(jnp.float32))
            return (highest, weight_sum, weighted)
        highest, weight_sum, weighted = lax.map(one_subset, grouped)
        overall = lax.optimization_barrier(jnp.max(highest, axis=0))
        factor = jnp.exp(highest - overall)
        merged = lax.optimization_barrier(jnp.sum(factor[..., None] * weighted, axis=0)) / lax.optimization_barrier(jnp.sum(factor * weight_sum, axis=0))[..., None]
        return merged.astype(jnp.bfloat16).reshape(TOK, H * DV)
    blocks = (query_content.reshape(N_SP, TOK, H, DN), query_turned.reshape(N_SP, TOK, H, DR), places.reshape(N_SP, TOK))
    head_out = lax.map(one_block, blocks).reshape(SEQ, H * DV)
    mixed_rows = (residual.astype(jnp.float32) + jnp.dot(head_out, out_proj, preferred_element_type=jnp.float32)).astype(jnp.bfloat16)
    mixed_rows = lax.optimization_barrier(mixed_rows)
    normed_rows = norm_round(mixed_rows, mixer_gain)
    hidden = (jax.nn.silu(jnp.dot(normed_rows, gate_proj, preferred_element_type=jnp.float32)) * jnp.dot(normed_rows, up_proj, preferred_element_type=jnp.float32)).astype(jnp.bfloat16)
    return (mixed_rows.astype(jnp.float32) + jnp.dot(hidden, down_proj, preferred_element_type=jnp.float32)).astype(jnp.bfloat16)
```

```python
import math

import jax
import jax.numpy as jnp
from jax import lax
from jax.experimental import pallas as pl
from jax.experimental.pallas import tpu as pltpu
from jax.sharding import Mesh, PartitionSpec as P

H = 8
DN = 128
DR = 64
DV = 128
SPAN = 64
NZ, NY, NX, NC = 16, 4, 4, 2
TOK = 192
HALF = TOK // 2
KEYS = 1536
PAD = 208

epsilon = 1e-06
masked_score = -1e30
LOG2E = 1.4426950408889634
VMEM_LIMIT = 60 * 1024 * 1024


def norm_round(inputs, scales):
    widened = inputs.astype(jnp.float32)
    factor = lax.rsqrt(jnp.mean(widened * widened, axis=-1, keepdims=True) + epsilon)
    return (widened * factor * scales).astype(jnp.bfloat16)


def tables(places):
    inverse = 10000.0 ** (-jnp.arange(0, DR, 2, dtype=jnp.float32) / DR)
    angles = places.astype(jnp.float32)[:, None] * inverse[None, :]
    return jnp.cos(angles), jnp.sin(angles)


def rotate_rows(inputs, places):
    cosine, sine = tables(places)
    widened = inputs.astype(jnp.float32)
    a, b = widened[:, : DR // 2], widened[:, DR // 2 :]
    return jnp.concatenate([a * cosine - b * sine, b * cosine + a * sine], axis=-1).astype(
        jnp.bfloat16
    )


def attend_kernel(q_ref, qr_ref, cos_ref, sin_ref, lat_ref, seg_ref, w_ref, out_ref, key_ref):
    scale = LOG2E / math.sqrt(DN + DR)
    step = pl.program_id(0)

    @pl.when(step == 0)
    def _():
        lane = lax.broadcasted_iota(jnp.int32, (KEYS, 64), 1)
        mask = jnp.where(seg_ref[:, :64] > lane, masked_score, 0.0)
        mask = jnp.where(lane < TOK // SPAN, mask, 0.0).astype(jnp.bfloat16)
        key_ref[:, DN : DN + DR] = lat_ref[:, 256:320]
        key_ref[:, DN + DR :] = mask

    turned = qr_ref[...].astype(jnp.float32)
    lane = lax.broadcasted_iota(jnp.int32, turned.shape, 1)
    first = lane % DR < DR // 2
    swapped = jnp.where(
        first, pltpu.roll(turned, 2 * DR - DR // 2, 1), pltpu.roll(turned, DR // 2, 1)
    )
    signed = jnp.where(first, -swapped, swapped)
    turned = (turned * cos_ref[...] + signed * sin_ref[...]).astype(jnp.bfloat16)
    row = lax.broadcasted_iota(jnp.int32, (TOK, 64), 0)
    col = lax.broadcasted_iota(jnp.int32, (TOK, 64), 1)
    segment = jnp.where(row // SPAN == col, 1.0, 0.0).astype(jnp.bfloat16)
    normed = lat_ref[:, :256]
    keys = jnp.dot(normed, w_ref[:256], preferred_element_type=jnp.float32).astype(jnp.bfloat16)
    values = jnp.dot(normed, w_ref[256:], preferred_element_type=jnp.float32).astype(jnp.bfloat16)
    ones = jnp.ones((KEYS, 128), jnp.bfloat16)
    r128 = lax.broadcasted_iota(jnp.int32, (128, 128), 0)
    c128 = lax.broadcasted_iota(jnp.int32, (128, 128), 1)
    r64 = lax.broadcasted_iota(jnp.int32, (64, 128), 0)
    c64 = lax.broadcasted_iota(jnp.int32, (64, 128), 1)
    for h in range(2):
        key_ref[:, :DN] = keys[:, h * DN : (h + 1) * DN]
        query = jnp.concatenate(
            [q_ref[:, h * DN : (h + 1) * DN], turned[:, h * DR : (h + 1) * DR], segment], axis=1
        )
        scores = lax.dot_general(
            query, key_ref[...], (((1,), (1,)), ((), ())), preferred_element_type=jnp.float32
        )
        highest = jnp.max(scores, axis=1, keepdims=True) * scale
        weights = jnp.exp2(scores * scale - highest).astype(jnp.bfloat16)
        both = jnp.concatenate([values[:, h * DV : (h + 1) * DV], ones], axis=1)
        sums = jnp.dot(weights, both, preferred_element_type=jnp.float32)
        norm = sums[:, DV:]
        out_ref[h, :TOK, :] = (sums[:, :DV] / norm).astype(jnp.bfloat16)
        level = highest + jnp.log2(norm)
        upper = jnp.sum(jnp.where(r128 == c128, level[:128], 0.0), axis=0, keepdims=True)
        lower = jnp.sum(jnp.where(r64 == c64, level[128:], 0.0), axis=0, keepdims=True)
        rest = jnp.concatenate([upper, lower], axis=0)
        rows = []
        for _ in range(3):
            part = rest.astype(jnp.bfloat16).astype(jnp.float32)
            rows.append(part)
            rest = rest - part
        rows.append(jnp.zeros((PAD - TOK - 6, 128), jnp.float32))
        out_ref[h, TOK:, :] = jnp.concatenate(rows, axis=0).astype(jnp.bfloat16)


def attend(query, query_rotary, cosine, sine, lat, seg, weights):
    return pl.pallas_call(
        attend_kernel,
        grid=(H // 2,),
        in_specs=[
            pl.BlockSpec((TOK, 2 * DN), lambda i: (0, i)),
            pl.BlockSpec((TOK, 2 * DR), lambda i: (0, i)),
            pl.BlockSpec((TOK, 2 * DR), lambda i: (0, 0)),
            pl.BlockSpec((TOK, 2 * DR), lambda i: (0, 0)),
            pl.BlockSpec((KEYS, 320), lambda i: (0, 0)),
            pl.BlockSpec((KEYS, 128), lambda i: (0, 0)),
            pl.BlockSpec((512, 2 * DN), lambda i: (0, i)),
        ],
        out_specs=pl.BlockSpec((2, PAD, 128), lambda i: (i, 0, 0)),
        out_shape=jax.ShapeDtypeStruct((H, PAD, 128), jnp.bfloat16),
        scratch_shapes=[pltpu.VMEM((KEYS, 256), jnp.bfloat16)],
        compiler_params=pltpu.CompilerParams(
            dimension_semantics=("arbitrary",), vmem_limit_bytes=VMEM_LIMIT
        ),
        cost_estimate=pl.CostEstimate(
            flops=3_000_000_000, bytes_accessed=4_000_000, transcendentals=2_400_000
        ),
        name="attend",
    )(query, query_rotary, cosine, sine, lat, seg, weights)


def merge_kernel(in_ref, out_ref):
    levels = []
    for j in range(H):
        tail = in_ref[j, TOK:, :].astype(jnp.float32)
        levels.append(tail[0:2] + tail[2:4] + tail[4:6])
    top = levels[0]
    for level in levels[1:]:
        top = jnp.maximum(top, level)
    factors = [jnp.exp2(level - top) for level in levels]
    total = factors[0]
    for factor in factors[1:]:
        total = total + factor
    r128 = lax.broadcasted_iota(jnp.int32, (128, 128), 0)
    c128 = lax.broadcasted_iota(jnp.int32, (128, 128), 1)
    acc = jnp.zeros((TOK, 128), jnp.float32)
    for j in range(H):
        share = factors[j] / total
        upper = jnp.sum(jnp.where(r128 == c128, share[0:1], 0.0), axis=1, keepdims=True)
        lower = jnp.sum(
            jnp.where(r128[:64] == c128[:64], share[1:2], 0.0), axis=1, keepdims=True
        )
        column = jnp.concatenate([upper, lower], axis=0)
        acc = acc + column * in_ref[j, :TOK, :].astype(jnp.float32)
    out_ref[...] = acc.astype(jnp.bfloat16)


def merge(parts):
    return pl.pallas_call(
        merge_kernel,
        out_shape=jax.ShapeDtypeStruct((TOK, 128), jnp.bfloat16),
        compiler_params=pltpu.CompilerParams(vmem_limit_bytes=VMEM_LIMIT),
        cost_estimate=pl.CostEstimate(flops=1_000_000, bytes_accessed=500_000, transcendentals=3000),
        name="merge",
    )(parts)


def mix_kernel(rows_ref, gain_ref, w_ref, out_ref, n_ref, g_ref, u_ref, d_ref):
    for z in range(NZ):
        for c in range(NC):
            block = slice(c * 176, (c + 1) * 176)
            lanes = slice(z * 128, (z + 1) * 128)
            g_ref[block, lanes] = w_ref[z, c, 0:176, :]
            u_ref[block, lanes] = w_ref[z, c, 176:352, :]
            d_ref[block, lanes] = w_ref[z, c, 352:528, :]
    for y in range(NY):
        square = jnp.zeros((HALF, 256), jnp.float32)
        for f in range(H):
            piece = rows_ref[y * H + f].astype(jnp.float32)
            square = square + piece * piece
        factor = lax.rsqrt(jnp.sum(square, axis=1, keepdims=True) / 2048.0 + epsilon)
        for f in range(H):
            piece = rows_ref[y * H + f].astype(jnp.float32)
            n_ref[y * HALF : (y + 1) * HALF, f * 256 : (f + 1) * 256] = (
                piece * factor * gain_ref[:, f * 256 : (f + 1) * 256]
            ).astype(jnp.bfloat16)
    dims = (((1,), (1,)), ((), ()))
    gate = lax.dot_general(n_ref[...], g_ref[...], dims, preferred_element_type=jnp.float32)
    up = lax.dot_general(n_ref[...], u_ref[...], dims, preferred_element_type=jnp.float32)
    hidden = (gate / (1.0 + jnp.exp(-gate)) * up).astype(jnp.bfloat16)
    for f in range(H):
        part = jnp.dot(
            hidden, d_ref[:, f * 256 : (f + 1) * 256], preferred_element_type=jnp.float32
        ).astype(jnp.bfloat16)
        for y in range(NY):
            out_ref[y * H + f] = part[y * HALF : (y + 1) * HALF]


def mix(rows, gain, weights):
    return pl.pallas_call(
        mix_kernel,
        out_shape=jax.ShapeDtypeStruct((NY * H, HALF, 256), jnp.bfloat16),
        scratch_shapes=[
            pltpu.VMEM((NY * HALF, 2048), jnp.bfloat16),
            pltpu.VMEM((352, 2048), jnp.bfloat16),
            pltpu.VMEM((352, 2048), jnp.bfloat16),
            pltpu.VMEM((352, 2048), jnp.bfloat16),
        ],
        compiler_params=pltpu.CompilerParams(vmem_limit_bytes=VMEM_LIMIT),
        cost_estimate=pl.CostEstimate(
            flops=1_700_000_000, bytes_accessed=8_000_000, transcendentals=140_000
        ),
        name="mix",
    )(rows, gain, weights)


def from_everyone(x, axis, count):
    copies = jnp.broadcast_to(x, (count, *x.shape))
    return lax.all_to_all(copies, axis, split_axis=0, concat_axis=0, tiled=True)


def shards(
    query_content,
    query_rotary,
    latents,
    key_rotary,
    latent_gain,
    key_up,
    value_up,
    out_proj,
    residual,
    mixer_gain,
    gate_proj,
    up_proj,
    down_proj,
):
    zi, yi = lax.axis_index("z"), lax.axis_index("y")
    sp_index = zi * NY + yi
    tp_index = lax.axis_index("x") * NC + lax.axis_index("c")

    kv = lax.all_gather(
        jnp.concatenate([key_up, value_up], axis=0), ("x", "c"), axis=1, tiled=True
    )

    own_places = (sp_index * 8 + tp_index) * 24 + jnp.arange(24, dtype=jnp.int32)
    own = jnp.concatenate(
        [norm_round(latents, latent_gain), rotate_rows(key_rotary, own_places)], axis=1
    )
    lat = from_everyone(own, "z", NZ).reshape(NZ * 24, 320)

    stacked = jnp.stack([gate_proj, up_proj, down_proj.T])
    slices = stacked.reshape(3, 32, NY, 176).transpose(2, 1, 0, 3).reshape(NY, 32, 528)
    slices, lat = lax.optimization_barrier((slices, lat))
    slices = lax.all_to_all(slices, "y", split_axis=0, concat_axis=0, tiled=True)
    slices, lat = lax.optimization_barrier((slices, lat))
    own_slice = slices.reshape(128, 528).T
    mixer = lax.all_gather(own_slice, ("z", "c"), axis=0, tiled=False).reshape(NZ, NC, 528, 128)

    lat = lax.all_gather(lat, "y", axis=0, tiled=True)

    index = jnp.arange(KEYS, dtype=jnp.int32)
    y_of, z_of, i_of = index // 384, index // 24 % NZ, index % 24
    key_segment = (((z_of * NY + y_of) * 8 + tp_index) * 24 + i_of) // SPAN
    seg = jnp.broadcast_to((key_segment - sp_index * (TOK // SPAN))[:, None], (KEYS, 128))
    cosine, sine = tables(sp_index * TOK + jnp.arange(TOK, dtype=jnp.int32))
    cosine, sine = (jnp.concatenate([t] * 4, axis=1) for t in (cosine, sine))

    parts = attend(query_content, query_rotary, cosine, sine, lat, seg, kv)
    parts = lax.all_to_all(parts, ("x", "c"), split_axis=0, concat_axis=0, tiled=True)
    attended = lax.all_gather(merge(parts), ("x", "c"), axis=1, tiled=True)
    mixed_rows = (
        residual.astype(jnp.float32)
        + jnp.dot(attended, out_proj, preferred_element_type=jnp.float32)
    ).astype(jnp.bfloat16)

    halves = mixed_rows.reshape(NC, HALF, 256)
    sent = jnp.broadcast_to(halves, (NY * NX, NC, HALF, 256)).reshape(32, HALF, 256)
    rows = lax.all_to_all(sent, ("y", "x", "c"), split_axis=0, concat_axis=0, tiled=True)
    partial_sums = mix(rows, mixer_gain.reshape(1, -1), mixer)
    arrived = lax.all_to_all(
        partial_sums, ("y", "x", "c"), split_axis=0, concat_axis=0, tiled=True
    )
    summed = arrived.reshape(NY * NX, TOK, 256).astype(jnp.float32).sum(axis=0)
    return (mixed_rows.astype(jnp.float32) + summed).astype(jnp.bfloat16)


def solution(mesh):
    fine = Mesh(mesh.devices.reshape(NZ, NY, NX, NC), ("z", "y", "x", "c"))
    sp, tp = ("z", "y"), ("x", "c")
    return jax.shard_map(
        shards,
        mesh=fine,
        in_specs=(
            P(sp, None),
            P(sp, None),
            P((*sp, *tp), None),
            P((*sp, *tp), None),
            P(),
            P(None, tp),
            P(None, tp),
            P(None, tp),
            P(sp, tp),
            P(),
            P(sp, tp),
            P(sp, tp),
            P(tp, sp),
        ),
        out_specs=P(sp, tp),
        check_vma=False,
    )
```

```python
import math

import jax
import jax.numpy as jnp
from jax import lax
from jax.experimental import pallas as pl
from jax.experimental.pallas import tpu as pltpu
from jax.sharding import Mesh, PartitionSpec as P


H = 8
DN = 128
DR = 64
DV = 128
SPAN = 64
NZ, NY, NX, NC = 16, 4, 4, 2
TOK = 192
HALF = TOK // 2
KEYS = 1536
PAD = 208
GROUP = 4

epsilon = 1e-06
masked_score = -1e30
LOG2E = 1.4426950408889634


def tables(places):
    inverse = 10000.0 ** (-jnp.arange(0, DR, 2, dtype=jnp.float32) / DR)
    angles = places.astype(jnp.float32)[:, None] * inverse[None, :]
    return jnp.cos(angles), jnp.sin(angles)


def prepare_kernel(lat_ref, rot_ref, gain_ref, cos_ref, sin_ref, k_ref, v_ref, out_ref, kv_ref):
    kv_ref[:, :DN] = k_ref[...]
    kv_ref[:, DN:] = v_ref[...]
    widened = lat_ref[...].astype(jnp.float32)
    factor = lax.rsqrt(jnp.mean(widened * widened, axis=-1, keepdims=True) + epsilon)
    normed = (widened * factor * gain_ref[...]).astype(jnp.bfloat16)
    widened = rot_ref[...].astype(jnp.float32)
    a, b = widened[:, : DR // 2], widened[:, DR // 2 :]
    cosine, sine = cos_ref[...], sin_ref[...]
    turned = jnp.concatenate([a * cosine - b * sine, b * cosine + a * sine], axis=-1)
    turned = turned.astype(jnp.bfloat16)
    for z in range(NZ):
        out_ref[z, :, :256] = normed
        out_ref[z, :, 256:] = turned


def prepare(*inputs):
    return pl.pallas_call(
        prepare_kernel,
        out_shape=(
            jax.ShapeDtypeStruct((NZ, 24, 320), jnp.bfloat16),
            jax.ShapeDtypeStruct((256, 256), jnp.bfloat16),
        ),
        compiler_params=pltpu.CompilerParams(vmem_limit_bytes=4 * 1024 * 1024),
        cost_estimate=pl.CostEstimate(flops=100_000, bytes_accessed=300_000, transcendentals=24),
        name="prepare",
    )(*inputs)


def attend_kernel(q_ref, qr_ref, cos_ref, sin_ref, lat_ref, seg_ref, w_ref, out_ref, key_ref):
    scale = LOG2E / math.sqrt(DN + DR)

    @pl.when(pl.program_id(0) == 0)
    def _():
        lane = lax.broadcasted_iota(jnp.int32, (KEYS, 64), 1)
        mask = jnp.where(seg_ref[:, :64] > lane, masked_score, 0.0)
        mask = jnp.where(lane < TOK // SPAN, mask, 0.0).astype(jnp.bfloat16)
        for h in range(GROUP):
            key_ref[h, :, DN : DN + DR] = lat_ref[:, 256:320]
            key_ref[h, :, DN + DR :] = mask

    turned = qr_ref[...].astype(jnp.float32)
    lane = lax.broadcasted_iota(jnp.int32, turned.shape, 1)
    first = lane % DR < DR // 2
    swapped = jnp.where(
        first, pltpu.roll(turned, GROUP * DR - DR // 2, 1), pltpu.roll(turned, DR // 2, 1)
    )
    signed = jnp.where(first, -swapped, swapped)
    cosine = jnp.concatenate([cos_ref[...]] * (GROUP // 2), axis=1)
    sine = jnp.concatenate([sin_ref[...]] * (GROUP // 2), axis=1)
    turned = (turned * cosine + signed * sine).astype(jnp.bfloat16)
    row = lax.broadcasted_iota(jnp.int32, (TOK, 64), 0)
    col = lax.broadcasted_iota(jnp.int32, (TOK, 64), 1)
    segment = jnp.where(row // SPAN == col, 1.0, 0.0).astype(jnp.bfloat16)
    normed = lat_ref[:, :256]
    ones = jnp.ones((KEYS, 128), jnp.bfloat16)
    r128 = lax.broadcasted_iota(jnp.int32, (128, 128), 0)
    c128 = lax.broadcasted_iota(jnp.int32, (128, 128), 1)
    for h in range(GROUP):
        pair = jnp.dot(normed, w_ref[h], preferred_element_type=jnp.float32).astype(jnp.bfloat16)
        query = jnp.concatenate(
            [q_ref[:, h * DN : (h + 1) * DN], turned[:, h * DR : (h + 1) * DR], segment], axis=1
        )
        key_ref[h, :, :DN] = pair[:, :DN]
        scores = lax.dot_general(
            query, key_ref[h], (((1,), (1,)), ((), ())), preferred_element_type=jnp.float32
        )
        highest = jnp.max(scores, axis=1, keepdims=True) * scale
        weights = jnp.exp2(scores * scale - highest).astype(jnp.bfloat16)
        both = jnp.concatenate([pair[:, DN:], ones], axis=1)
        sums = jnp.dot(weights, both, preferred_element_type=jnp.float32)
        norm = sums[:, DV:]
        out_ref[h, :TOK, :] = (sums[:, :DV] / norm).astype(jnp.bfloat16)
        level = highest + jnp.log2(norm)
        upper = jnp.sum(jnp.where(r128 == c128, level[:128], 0.0), axis=0, keepdims=True)
        lower = jnp.sum(
            jnp.where(r128[:64] == c128[:64], level[128:], 0.0), axis=0, keepdims=True
        )
        rest = jnp.concatenate([upper, lower], axis=0)
        rows = []
        for _ in range(3):
            part = rest.astype(jnp.bfloat16).astype(jnp.float32)
            rows.append(part)
            rest = rest - part
        rows.append(jnp.zeros((PAD - TOK - 6, 128), jnp.float32))
        out_ref[h, TOK:, :] = jnp.concatenate(rows, axis=0).astype(jnp.bfloat16)


def attend(query, query_rotary, cosine, sine, lat, seg, weights):
    return pl.pallas_call(
        attend_kernel,
        grid=(H // GROUP,),
        in_specs=[
            pl.BlockSpec((TOK, GROUP * DN), lambda i: (0, i)),
            pl.BlockSpec((TOK, GROUP * DR), lambda i: (0, i)),
            pl.BlockSpec((TOK, 2 * DR), lambda i: (0, 0)),
            pl.BlockSpec((TOK, 2 * DR), lambda i: (0, 0)),
            pl.BlockSpec((KEYS, 320), lambda i: (0, 0)),
            pl.BlockSpec((KEYS, 128), lambda i: (0, 0)),
            pl.BlockSpec((GROUP, 256, 256), lambda i: (i, 0, 0)),
        ],
        out_specs=pl.BlockSpec((GROUP, PAD, 128), lambda i: (i, 0, 0)),
        out_shape=jax.ShapeDtypeStruct((H, PAD, 128), jnp.bfloat16),
        scratch_shapes=[pltpu.VMEM((GROUP, KEYS, 256), jnp.bfloat16)],
        compiler_params=pltpu.CompilerParams(
            dimension_semantics=("arbitrary",), vmem_limit_bytes=24 * 1024 * 1024
        ),
        cost_estimate=pl.CostEstimate(
            flops=3_000_000_000, bytes_accessed=4_000_000, transcendentals=2_400_000
        ),
        name="attend",
    )(query, query_rotary, cosine, sine, lat, seg, weights)


def merge_kernel(in_ref, out_ref):
    levels = []
    for j in range(H):
        tail = in_ref[j, TOK:, :].astype(jnp.float32)
        levels.append(tail[0:2] + tail[2:4] + tail[4:6])
    top = levels[0]
    for level in levels[1:]:
        top = jnp.maximum(top, level)
    factors = [jnp.exp2(level - top) for level in levels]
    total = factors[0]
    for factor in factors[1:]:
        total = total + factor
    r128 = lax.broadcasted_iota(jnp.int32, (128, 128), 0)
    c128 = lax.broadcasted_iota(jnp.int32, (128, 128), 1)
    acc = jnp.zeros((TOK, 128), jnp.float32)
    for j in range(H):
        share = factors[j] / total
        upper = jnp.sum(jnp.where(r128 == c128, share[0:1], 0.0), axis=1, keepdims=True)
        lower = jnp.sum(
            jnp.where(r128[:64] == c128[:64], share[1:2], 0.0), axis=1, keepdims=True
        )
        column = jnp.concatenate([upper, lower], axis=0)
        acc = acc + column * in_ref[j, :TOK, :].astype(jnp.float32)
    out_ref[...] = acc.astype(jnp.bfloat16)


def merge(parts):
    return pl.pallas_call(
        merge_kernel,
        out_shape=jax.ShapeDtypeStruct((TOK, 128), jnp.bfloat16),
        compiler_params=pltpu.CompilerParams(vmem_limit_bytes=8 * 1024 * 1024),
        cost_estimate=pl.CostEstimate(flops=1_000_000, bytes_accessed=500_000, transcendentals=3000),
        name="merge",
    )(parts)


def mix_kernel(rows_ref, gain_ref, w_hbm, out_ref, n_ref, w_ref, sem):
    copies = [
        pltpu.make_async_copy(w_hbm.at[z], w_ref.at[:, pl.ds(z * 128, 128)], sem.at[z])
        for z in range(NZ)
    ]
    for copy in copies:
        copy.start()
    for y in range(NY):
        square = jnp.zeros((HALF, 256), jnp.float32)
        for f in range(H):
            piece = rows_ref[y * H + f].astype(jnp.float32)
            square = square + piece * piece
        factor = lax.rsqrt(jnp.sum(square, axis=1, keepdims=True) / 2048.0 + epsilon)
        for f in range(H):
            piece = rows_ref[y * H + f].astype(jnp.float32)
            n_ref[y * HALF : (y + 1) * HALF, f * 256 : (f + 1) * 256] = (
                piece * factor * gain_ref[:, f * 256 : (f + 1) * 256]
            ).astype(jnp.bfloat16)
    for copy in copies:
        copy.wait()
    dims = (((1,), (1,)), ((), ()))
    hidden = []
    for c in range(NC):
        gate = lax.dot_general(
            n_ref[...], w_ref[c * 528 : c * 528 + 176], dims, preferred_element_type=jnp.float32
        )
        up = lax.dot_general(
            n_ref[...], w_ref[c * 528 + 176 : c * 528 + 352], dims,
            preferred_element_type=jnp.float32,
        )
        hidden.append((gate / (1.0 + jnp.exp(-gate)) * up).astype(jnp.bfloat16))
    for f in range(H):
        lanes = slice(f * 256, (f + 1) * 256)
        part = sum(
            jnp.dot(
                hidden[c], w_ref[c * 528 + 352 : (c + 1) * 528, lanes],
                preferred_element_type=jnp.float32,
            )
            for c in range(NC)
        ).astype(jnp.bfloat16)
        for y in range(NY):
            out_ref[y * H + f] = part[y * HALF : (y + 1) * HALF]


def mix(rows, gain, weights):
    whole = pl.BlockSpec(memory_space=pltpu.VMEM)
    return pl.pallas_call(
        mix_kernel,
        in_specs=[whole, whole, pl.BlockSpec(memory_space=pltpu.HBM)],
        out_specs=whole,
        out_shape=jax.ShapeDtypeStruct((NY * H, HALF, 256), jnp.bfloat16),
        scratch_shapes=[
            pltpu.VMEM((NY * HALF, 2048), jnp.bfloat16),
            pltpu.VMEM((1056, 2048), jnp.bfloat16),
            pltpu.SemaphoreType.DMA((NZ,)),
        ],
        compiler_params=pltpu.CompilerParams(vmem_limit_bytes=63_200_000),
        cost_estimate=pl.CostEstimate(
            flops=1_700_000_000, bytes_accessed=8_000_000, transcendentals=140_000
        ),
        name="mix",
    )(rows, gain, weights)


def project_kernel(heads_ref, w_ref, res_ref, mixed_ref, sent_ref):
    heads = jnp.concatenate([heads_ref[h] for h in range(H)], axis=1)
    mixed = (
        res_ref[...].astype(jnp.float32)
        + jnp.dot(heads, w_ref[...], preferred_element_type=jnp.float32)
    ).astype(jnp.bfloat16)
    mixed_ref[...] = mixed
    for d in range(NY * NX):
        for c in range(NC):
            sent_ref[d * NC + c] = mixed[c * HALF : (c + 1) * HALF]


def project(heads, weights, residual):
    return pl.pallas_call(
        project_kernel,
        out_shape=(
            jax.ShapeDtypeStruct((TOK, 256), jnp.bfloat16),
            jax.ShapeDtypeStruct((NY * NX * NC, HALF, 256), jnp.bfloat16),
        ),
        compiler_params=pltpu.CompilerParams(vmem_limit_bytes=12 * 1024 * 1024),
        cost_estimate=pl.CostEstimate(
            flops=100_000_000, bytes_accessed=3_000_000, transcendentals=0
        ),
        name="project",
    )(heads, weights, residual)


def layer(
    query_content,
    query_rotary,
    latents,
    key_rotary,
    latent_gain,
    key_up,
    value_up,
    out_proj,
    residual,
    mixer_gain,
    gate_proj,
    up_proj,
    down_proj,
):
    zi, yi = lax.axis_index("z"), lax.axis_index("y")
    sp_index = zi * NY + yi
    tp_index = lax.axis_index("x") * NC + lax.axis_index("c")

    own_places = (sp_index * 8 + tp_index) * 24 + jnp.arange(24, dtype=jnp.int32)
    cosine, sine = tables(own_places)
    own, kv = prepare(
        latents, key_rotary, latent_gain.reshape(1, -1), cosine, sine, key_up, value_up
    )
    kv = lax.all_gather(kv, ("x", "c"), axis=0, tiled=False)

    stacked = jnp.stack([gate_proj, up_proj, down_proj.T])
    slices = stacked.reshape(3, 32, NY, 176).transpose(2, 1, 0, 3).reshape(NY, 32, 528)
    ahead = lax.dynamic_slice_in_dim(jnp.concatenate([slices, slices]), yi, NY, axis=0)
    lat = lax.all_to_all(own, "z", split_axis=0, concat_axis=0, tiled=True)
    lat = lat.reshape(NZ * 24, 320)
    back = [ahead[0]] + [
        lax.ppermute(ahead[s], "y", [(i, (i + s) % NY) for i in range(NY)]) for s in range(1, NY)
    ]
    turn = jnp.stack(back[::-1] * 2)
    own_slice = lax.dynamic_slice_in_dim(turn, NY - 1 - yi, NY, axis=0).reshape(128, 528).T
    mixer = lax.all_gather(own_slice, ("z", "c"), axis=0, tiled=True).reshape(
        NZ, NC * 528, 128
    )

    lat = lax.all_gather(lat, "y", axis=0, tiled=True)

    index = jnp.arange(KEYS, dtype=jnp.int32)
    y_of, z_of, i_of = index // 384, index // 24 % NZ, index % 24
    key_segment = (((z_of * NY + y_of) * 8 + tp_index) * 24 + i_of) // SPAN
    seg = jnp.broadcast_to((key_segment - sp_index * (TOK // SPAN))[:, None], (KEYS, 128))
    cosine, sine = tables(sp_index * TOK + jnp.arange(TOK, dtype=jnp.int32))
    cosine, sine = (jnp.concatenate([t] * 4, axis=1) for t in (cosine, sine))

    parts = attend(query_content, query_rotary, cosine, sine, lat, seg, kv)
    parts = lax.all_to_all(parts, ("x", "c"), split_axis=0, concat_axis=0, tiled=True)
    heads = lax.all_gather(merge(parts), ("x", "c"), axis=0, tiled=False)
    mixed_rows, sent = project(heads, out_proj, residual)
    rows = lax.all_to_all(sent, ("y", "x", "c"), split_axis=0, concat_axis=0, tiled=True)
    partial_sums = mix(rows, mixer_gain.reshape(1, -1), mixer)
    arrived = lax.all_to_all(
        partial_sums, ("y", "x", "c"), split_axis=0, concat_axis=0, tiled=True
    )
    summed = arrived.reshape(NY * NX, TOK, 256).astype(jnp.float32).sum(axis=0)
    return (mixed_rows.astype(jnp.float32) + summed).astype(jnp.bfloat16)


def solution(mesh):
    fine = Mesh(mesh.devices.reshape(NZ, NY, NX, NC), ("z", "y", "x", "c"))
    sp, tp = ("z", "y"), ("x", "c")
    return jax.shard_map(
        layer,
        mesh=fine,
        in_specs=(
            P(sp, None),
            P(sp, None),
            P((*sp, *tp), None),
            P((*sp, *tp), None),
            P(),
            P(None, tp),
            P(None, tp),
            P(None, tp),
            P(sp, tp),
            P(),
            P(sp, tp),
            P(sp, tp),
            P(tp, sp),
        ),
        out_specs=P(sp, tp),
        check_vma=False,
    )
```

```python
import math

import jax
import jax.numpy as jnp
from jax import lax
from jax.experimental import pallas as pl
from jax.experimental.pallas import tpu as pltpu
from jax.sharding import Mesh, PartitionSpec as P


H = 8
DN = 128
DR = 64
DV = 128
SPAN = 64
NZ, NY, NX, NC = 16, 4, 4, 2
TOK = 192
HALF = TOK // 2
KEYS = 1536
PAD = 208
GROUP = 4

epsilon = 1e-06
masked_score = -1e30
LOG2E = 1.4426950408889634


def tables(places):
    inverse = 10000.0 ** (-jnp.arange(0, DR, 2, dtype=jnp.float32) / DR)
    angles = places.astype(jnp.float32)[:, None] * inverse[None, :]
    return jnp.cos(angles), jnp.sin(angles)


def prepare_kernel(
    y_ref, lat_ref, rot_ref, gain_ref, cos_ref, sin_ref, k_ref, v_ref, gate_ref, up_ref, down_ref,
    out_ref, kv_ref, cut_ref,
):
    for k in range(NY):
        block = slice(k * 176, (k + 1) * 176)
        cut_ref[(k + NY - y_ref[0]) % NY] = jnp.concatenate(
            [gate_ref[:, block], up_ref[:, block], down_ref[:, block]], axis=1
        )
    kv_ref[:, :DN] = k_ref[...]
    kv_ref[:, DN:] = v_ref[...]
    widened = lat_ref[...].astype(jnp.float32)
    factor = lax.rsqrt(jnp.mean(widened * widened, axis=-1, keepdims=True) + epsilon)
    normed = (widened * factor * gain_ref[...]).astype(jnp.bfloat16)
    widened = rot_ref[...].astype(jnp.float32)
    a, b = widened[:, : DR // 2], widened[:, DR // 2 :]
    cosine, sine = cos_ref[...], sin_ref[...]
    turned = jnp.concatenate([a * cosine - b * sine, b * cosine + a * sine], axis=-1)
    turned = turned.astype(jnp.bfloat16)
    for z in range(NZ):
        out_ref[z, :, :256] = normed
        out_ref[z, :, 256:] = turned


def prepare(*inputs):
    return pl.pallas_call(
        prepare_kernel,
        out_shape=(
            jax.ShapeDtypeStruct((NZ, 24, 320), jnp.bfloat16),
            jax.ShapeDtypeStruct((256, 256), jnp.bfloat16),
            jax.ShapeDtypeStruct((NY, 32, 528), jnp.bfloat16),
        ),
        in_specs=[pl.BlockSpec(memory_space=pltpu.SMEM)]
        + [pl.BlockSpec(memory_space=pltpu.VMEM)] * 10,
        compiler_params=pltpu.CompilerParams(vmem_limit_bytes=66_900_000),
        cost_estimate=pl.CostEstimate(flops=100_000, bytes_accessed=300_000, transcendentals=24),
        name="prepare",
    )(*inputs)


def put_kernel(y_ref, a_ref, b_ref, c_ref, d_ref, out_ref, all_ref):
    y = y_ref[0]
    for s, ref in enumerate((a_ref, b_ref, c_ref, d_ref)):
        all_ref[(y + NY - s) % NY, :, :528] = ref[...].astype(jnp.float32)
    for k in range(5):
        lanes = jnp.concatenate(
            [all_ref[r, :, k * 128 : (k + 1) * 128] for r in range(NY)], axis=0
        )
        rows = min(128, 528 - k * 128)
        out_ref[k * 128 : k * 128 + rows] = lanes.T[:rows].astype(jnp.bfloat16)


def put(y, *pieces):
    small = pl.BlockSpec(memory_space=pltpu.VMEM)
    return pl.pallas_call(
        put_kernel,
        in_specs=[pl.BlockSpec(memory_space=pltpu.SMEM), small, small, small, small],
        out_shape=jax.ShapeDtypeStruct((528, 128), jnp.bfloat16),
        scratch_shapes=[pltpu.VMEM((NY, 32, 640), jnp.float32)],
        compiler_params=pltpu.CompilerParams(vmem_limit_bytes=4 * 1024 * 1024),
        cost_estimate=pl.CostEstimate(flops=100_000, bytes_accessed=300_000, transcendentals=0),
        name="put",
    )(y, *pieces)


def attend_kernel(q_ref, qr_ref, cos_ref, sin_ref, lat_ref, seg_ref, w_ref, out_ref, key_ref):
    scale = LOG2E / math.sqrt(DN + DR)

    @pl.when(pl.program_id(0) == 0)
    def _():
        lane = lax.broadcasted_iota(jnp.int32, (KEYS, 64), 1)
        mask = jnp.where(seg_ref[:, :64] > lane, masked_score, 0.0)
        mask = jnp.where(lane < TOK // SPAN, mask, 0.0).astype(jnp.bfloat16)
        for h in range(GROUP):
            key_ref[h, :, DN : DN + DR] = lat_ref[:, 256:320]
            key_ref[h, :, DN + DR :] = mask

    turned = qr_ref[...].astype(jnp.float32)
    lane = lax.broadcasted_iota(jnp.int32, turned.shape, 1)
    first = lane % DR < DR // 2
    swapped = jnp.where(
        first, pltpu.roll(turned, GROUP * DR - DR // 2, 1), pltpu.roll(turned, DR // 2, 1)
    )
    signed = jnp.where(first, -swapped, swapped)
    cosine = jnp.concatenate([cos_ref[...]] * (GROUP // 2), axis=1)
    sine = jnp.concatenate([sin_ref[...]] * (GROUP // 2), axis=1)
    turned = (turned * cosine + signed * sine).astype(jnp.bfloat16)
    row = lax.broadcasted_iota(jnp.int32, (TOK, 64), 0)
    col = lax.broadcasted_iota(jnp.int32, (TOK, 64), 1)
    segment = jnp.where(row // SPAN == col, 1.0, 0.0).astype(jnp.bfloat16)
    normed = lat_ref[:, :256]
    ones = jnp.ones((KEYS, 128), jnp.bfloat16)
    r128 = lax.broadcasted_iota(jnp.int32, (128, 128), 0)
    c128 = lax.broadcasted_iota(jnp.int32, (128, 128), 1)
    for h in range(GROUP):
        pair = jnp.dot(normed, w_ref[h], preferred_element_type=jnp.float32).astype(jnp.bfloat16)
        query = jnp.concatenate(
            [q_ref[:, h * DN : (h + 1) * DN], turned[:, h * DR : (h + 1) * DR], segment], axis=1
        )
        key_ref[h, :, :DN] = pair[:, :DN]
        scores = lax.dot_general(
            query, key_ref[h], (((1,), (1,)), ((), ())), preferred_element_type=jnp.float32
        )
        highest = jnp.max(scores, axis=1, keepdims=True) * scale
        weights = jnp.exp2(scores * scale - highest).astype(jnp.bfloat16)
        both = jnp.concatenate([pair[:, DN:], ones], axis=1)
        sums = jnp.dot(weights, both, preferred_element_type=jnp.float32)
        norm = sums[:, DV:]
        out_ref[h, :TOK, :] = (sums[:, :DV] / norm).astype(jnp.bfloat16)
        level = highest + jnp.log2(norm)
        upper = jnp.sum(jnp.where(r128 == c128, level[:128], 0.0), axis=0, keepdims=True)
        lower = jnp.sum(
            jnp.where(r128[:64] == c128[:64], level[128:], 0.0), axis=0, keepdims=True
        )
        rest = jnp.concatenate([upper, lower], axis=0)
        rows = []
        for _ in range(3):
            part = rest.astype(jnp.bfloat16).astype(jnp.float32)
            rows.append(part)
            rest = rest - part
        rows.append(jnp.zeros((PAD - TOK - 6, 128), jnp.float32))
        out_ref[h, TOK:, :] = jnp.concatenate(rows, axis=0).astype(jnp.bfloat16)


def attend(query, query_rotary, cosine, sine, lat, seg, weights):
    return pl.pallas_call(
        attend_kernel,
        grid=(H // GROUP,),
        in_specs=[
            pl.BlockSpec((TOK, GROUP * DN), lambda i: (0, i)),
            pl.BlockSpec((TOK, GROUP * DR), lambda i: (0, i)),
            pl.BlockSpec((TOK, 2 * DR), lambda i: (0, 0)),
            pl.BlockSpec((TOK, 2 * DR), lambda i: (0, 0)),
            pl.BlockSpec((KEYS, 320), lambda i: (0, 0)),
            pl.BlockSpec((KEYS, 128), lambda i: (0, 0)),
            pl.BlockSpec((GROUP, 256, 256), lambda i: (i, 0, 0)),
        ],
        out_specs=pl.BlockSpec((GROUP, PAD, 128), lambda i: (i, 0, 0)),
        out_shape=jax.ShapeDtypeStruct((H, PAD, 128), jnp.bfloat16),
        scratch_shapes=[pltpu.VMEM((GROUP, KEYS, 256), jnp.bfloat16)],
        compiler_params=pltpu.CompilerParams(
            dimension_semantics=("arbitrary",), vmem_limit_bytes=24 * 1024 * 1024
        ),
        cost_estimate=pl.CostEstimate(
            flops=3_000_000_000, bytes_accessed=4_000_000, transcendentals=2_400_000
        ),
        name="attend",
    )(query, query_rotary, cosine, sine, lat, seg, weights)


def merge_kernel(in_ref, out_ref):
    levels = []
    for j in range(H):
        tail = in_ref[j, TOK:, :].astype(jnp.float32)
        levels.append(tail[0:2] + tail[2:4] + tail[4:6])
    top = levels[0]
    for level in levels[1:]:
        top = jnp.maximum(top, level)
    factors = [jnp.exp2(level - top) for level in levels]
    total = factors[0]
    for factor in factors[1:]:
        total = total + factor
    r128 = lax.broadcasted_iota(jnp.int32, (128, 128), 0)
    c128 = lax.broadcasted_iota(jnp.int32, (128, 128), 1)
    acc = jnp.zeros((TOK, 128), jnp.float32)
    for j in range(H):
        share = factors[j] / total
        upper = jnp.sum(jnp.where(r128 == c128, share[0:1], 0.0), axis=1, keepdims=True)
        lower = jnp.sum(
            jnp.where(r128[:64] == c128[:64], share[1:2], 0.0), axis=1, keepdims=True
        )
        column = jnp.concatenate([upper, lower], axis=0)
        acc = acc + column * in_ref[j, :TOK, :].astype(jnp.float32)
    merged = acc.astype(jnp.bfloat16)
    for j in range(H):
        out_ref[j] = merged


def merge(parts):
    return pl.pallas_call(
        merge_kernel,
        out_shape=jax.ShapeDtypeStruct((H, TOK, 128), jnp.bfloat16),
        compiler_params=pltpu.CompilerParams(vmem_limit_bytes=8 * 1024 * 1024),
        cost_estimate=pl.CostEstimate(flops=1_000_000, bytes_accessed=500_000, transcendentals=3000),
        name="merge",
    )(parts)


def mix_kernel(rows_ref, gain_ref, w_hbm, out_ref, n_ref, w_ref, sem):
    copies = [
        pltpu.make_async_copy(w_hbm.at[z], w_ref.at[:, pl.ds(z * 128, 128)], sem.at[z])
        for z in range(NZ)
    ]
    for copy in copies:
        copy.start()
    for y in range(NY):
        square = jnp.zeros((HALF, 256), jnp.float32)
        for f in range(H):
            piece = rows_ref[y * H + f].astype(jnp.float32)
            square = square + piece * piece
        factor = lax.rsqrt(jnp.sum(square, axis=1, keepdims=True) / 2048.0 + epsilon)
        for f in range(H):
            piece = rows_ref[y * H + f].astype(jnp.float32)
            n_ref[y * HALF : (y + 1) * HALF, f * 256 : (f + 1) * 256] = (
                piece * factor * gain_ref[:, f * 256 : (f + 1) * 256]
            ).astype(jnp.bfloat16)
    for copy in copies:
        copy.wait()
    dims = (((1,), (1,)), ((), ()))
    hidden = []
    for c in range(NC):
        gate = lax.dot_general(
            n_ref[...], w_ref[c * 528 : c * 528 + 176], dims, preferred_element_type=jnp.float32
        )
        up = lax.dot_general(
            n_ref[...], w_ref[c * 528 + 176 : c * 528 + 352], dims,
            preferred_element_type=jnp.float32,
        )
        hidden.append((gate / (1.0 + jnp.exp(-gate)) * up).astype(jnp.bfloat16))
    for f in range(H):
        lanes = slice(f * 256, (f + 1) * 256)
        part = sum(
            jnp.dot(
                hidden[c], w_ref[c * 528 + 352 : (c + 1) * 528, lanes],
                preferred_element_type=jnp.float32,
            )
            for c in range(NC)
        ).astype(jnp.bfloat16)
        for y in range(NY):
            out_ref[y * H + f] = part[y * HALF : (y + 1) * HALF]


def mix(rows, gain, weights):
    whole = pl.BlockSpec(memory_space=pltpu.VMEM)
    return pl.pallas_call(
        mix_kernel,
        in_specs=[whole, whole, pl.BlockSpec(memory_space=pltpu.HBM)],
        out_specs=whole,
        out_shape=jax.ShapeDtypeStruct((NY * H, HALF, 256), jnp.bfloat16),
        scratch_shapes=[
            pltpu.VMEM((NY * HALF, 2048), jnp.bfloat16),
            pltpu.VMEM((1056, 2048), jnp.bfloat16),
            pltpu.SemaphoreType.DMA((NZ,)),
        ],
        compiler_params=pltpu.CompilerParams(vmem_limit_bytes=63_200_000),
        cost_estimate=pl.CostEstimate(
            flops=1_700_000_000, bytes_accessed=8_000_000, transcendentals=140_000
        ),
        name="mix",
    )(rows, gain, weights)


def project_kernel(heads_ref, w_ref, res_ref, mixed_ref, sent_ref):
    heads = jnp.concatenate([heads_ref[h] for h in range(H)], axis=1)
    mixed = (
        res_ref[...].astype(jnp.float32)
        + jnp.dot(heads, w_ref[...], preferred_element_type=jnp.float32)
    ).astype(jnp.bfloat16)
    mixed_ref[...] = mixed
    for d in range(NY * NX):
        for c in range(NC):
            sent_ref[d * NC + c] = mixed[c * HALF : (c + 1) * HALF]


def project(heads, weights, residual):
    return pl.pallas_call(
        project_kernel,
        out_shape=(
            jax.ShapeDtypeStruct((TOK, 256), jnp.bfloat16),
            jax.ShapeDtypeStruct((NY * NX * NC, HALF, 256), jnp.bfloat16),
        ),
        compiler_params=pltpu.CompilerParams(vmem_limit_bytes=12 * 1024 * 1024),
        cost_estimate=pl.CostEstimate(
            flops=100_000_000, bytes_accessed=3_000_000, transcendentals=0
        ),
        name="project",
    )(heads, weights, residual)


def layer(
    query_content,
    query_rotary,
    latents,
    key_rotary,
    latent_gain,
    key_up,
    value_up,
    out_proj,
    residual,
    mixer_gain,
    gate_proj,
    up_proj,
    down_proj,
):
    zi, yi = lax.axis_index("z"), lax.axis_index("y")
    sp_index = zi * NY + yi
    tp_index = lax.axis_index("x") * NC + lax.axis_index("c")

    own_places = (sp_index * 8 + tp_index) * 24 + jnp.arange(24, dtype=jnp.int32)
    cosine, sine = tables(own_places)
    y_word = yi.reshape(1).astype(jnp.int32)
    own, kv, ahead = prepare(
        y_word, latents, key_rotary, latent_gain.reshape(1, -1), cosine, sine, key_up, value_up,
        gate_proj, up_proj, down_proj.T,
    )
    kv = lax.all_gather(kv, ("x", "c"), axis=0, tiled=False)

    lat = lax.all_to_all(own, "z", split_axis=0, concat_axis=0, tiled=True)
    lat = lat.reshape(NZ * 24, 320)
    pieces = [ahead[s] for s in range(NY)]
    back = [
        lax.ppermute(pieces[s], "y", [(i, (i + s) % NY) for i in range(NY)]) for s in range(1, NY)
    ]
    own_slice = put(y_word, pieces[0], *back)
    mixer = lax.all_gather(own_slice, ("z", "c"), axis=0, tiled=True).reshape(
        NZ, NC * 528, 128
    )

    lat = lax.all_gather(lat, "y", axis=0, tiled=True)

    index = jnp.arange(KEYS, dtype=jnp.int32)
    y_of, z_of, i_of = index // 384, index // 24 % NZ, index % 24
    key_segment = (((z_of * NY + y_of) * 8 + tp_index) * 24 + i_of) // SPAN
    seg = jnp.broadcast_to((key_segment - sp_index * (TOK // SPAN))[:, None], (KEYS, 128))
    cosine, sine = tables(sp_index * TOK + jnp.arange(TOK, dtype=jnp.int32))
    cosine, sine = (jnp.concatenate([t] * 4, axis=1) for t in (cosine, sine))

    parts = attend(query_content, query_rotary, cosine, sine, lat, seg, kv)
    parts = lax.all_to_all(parts, ("x", "c"), split_axis=0, concat_axis=0, tiled=True)
    heads = lax.all_to_all(merge(parts), ("x", "c"), split_axis=0, concat_axis=0, tiled=True)
    mixed_rows, sent = project(heads, out_proj, residual)
    rows = lax.all_to_all(sent, ("y", "x", "c"), split_axis=0, concat_axis=0, tiled=True)
    partial_sums = mix(rows, mixer_gain.reshape(1, -1), mixer)
    arrived = lax.all_to_all(
        partial_sums, ("y", "x", "c"), split_axis=0, concat_axis=0, tiled=True
    )
    summed = arrived.reshape(NY * NX, TOK, 256).astype(jnp.float32).sum(axis=0)
    return (mixed_rows.astype(jnp.float32) + summed).astype(jnp.bfloat16)


def solution(mesh):
    fine = Mesh(mesh.devices.reshape(NZ, NY, NX, NC), ("z", "y", "x", "c"))
    sp, tp = ("z", "y"), ("x", "c")
    return jax.shard_map(
        layer,
        mesh=fine,
        in_specs=(
            P(sp, None),
            P(sp, None),
            P((*sp, *tp), None),
            P((*sp, *tp), None),
            P(),
            P(None, tp),
            P(None, tp),
            P(None, tp),
            P(sp, tp),
            P(),
            P(sp, tp),
            P(sp, tp),
            P(tp, sp),
        ),
        out_specs=P(sp, tp),
        check_vma=False,
    )
```

```python
import math

import jax
import jax.numpy as jnp
from jax import lax
from jax.experimental import pallas as pl
from jax.experimental.pallas import tpu as pltpu
from jax.sharding import Mesh, PartitionSpec as P


H = 8
DN = 128
DR = 64
DV = 128
SPAN = 64
NZ, NY, NX, NC = 16, 4, 4, 2
TOK = 192
HALF = TOK // 2
KEYS = 1536
PAD = 208
GROUP = 4
ROWS = KEYS // 3

epsilon = 1e-06
masked_score = -1e30
LOG2E = 1.4426950408889634


def tables(places):
    inverse = 10000.0 ** (-jnp.arange(0, DR, 2, dtype=jnp.float32) / DR)
    angles = places.astype(jnp.float32)[:, None] * inverse[None, :]
    return jnp.cos(angles), jnp.sin(angles)


def prepare_kernel(
    y_ref, lat_ref, rot_ref, gain_ref, cos_ref, sin_ref, k_ref, v_ref, gate_ref, up_ref, down_ref,
    out_ref, kv_ref, cut_ref,
):
    for k in range(NY):
        block = slice(k * 176, (k + 1) * 176)
        cut_ref[(k + NY - y_ref[0]) % NY] = jnp.concatenate(
            [gate_ref[:, block], up_ref[:, block], down_ref[:, block]], axis=1
        )
    kv_ref[:, :DN] = k_ref[...]
    kv_ref[:, DN:] = v_ref[...]
    widened = lat_ref[...].astype(jnp.float32)
    factor = lax.rsqrt(jnp.mean(widened * widened, axis=-1, keepdims=True) + epsilon)
    normed = (widened * factor * gain_ref[...]).astype(jnp.bfloat16)
    widened = rot_ref[...].astype(jnp.float32)
    a, b = widened[:, : DR // 2], widened[:, DR // 2 :]
    cosine, sine = cos_ref[...], sin_ref[...]
    turned = jnp.concatenate([a * cosine - b * sine, b * cosine + a * sine], axis=-1)
    turned = turned.astype(jnp.bfloat16)
    keys = [slice(j * 8, (j + 1) * 8) for j in range(3)]
    row = jnp.concatenate([normed[k] for k in keys] + [turned[k] for k in keys], axis=1)
    for z in range(NZ):
        out_ref[z] = row


def prepare(*inputs):
    return pl.pallas_call(
        prepare_kernel,
        out_shape=(
            jax.ShapeDtypeStruct((NZ, 8, 960), jnp.bfloat16),
            jax.ShapeDtypeStruct((256, 256), jnp.bfloat16),
            jax.ShapeDtypeStruct((NY, 32, 528), jnp.bfloat16),
        ),
        in_specs=[pl.BlockSpec(memory_space=pltpu.SMEM)]
        + [pl.BlockSpec(memory_space=pltpu.VMEM)] * 10,
        compiler_params=pltpu.CompilerParams(vmem_limit_bytes=66_900_000),
        cost_estimate=pl.CostEstimate(flops=100_000, bytes_accessed=300_000, transcendentals=24),
        name="prepare",
    )(*inputs)


def put_kernel(y_ref, a_ref, b_ref, c_ref, d_ref, out_ref, all_ref):
    y = y_ref[0]
    for s, ref in enumerate((a_ref, b_ref, c_ref, d_ref)):
        all_ref[(y + NY - s) % NY, :, :528] = ref[...].astype(jnp.float32)
    for k in range(5):
        lanes = jnp.concatenate(
            [all_ref[r, :, k * 128 : (k + 1) * 128] for r in range(NY)], axis=0
        )
        rows = min(128, 528 - k * 128)
        out_ref[k * 128 : k * 128 + rows] = lanes.T[:rows].astype(jnp.bfloat16)


def put(y, *pieces):
    small = pl.BlockSpec(memory_space=pltpu.VMEM)
    return pl.pallas_call(
        put_kernel,
        in_specs=[pl.BlockSpec(memory_space=pltpu.SMEM), small, small, small, small],
        out_shape=jax.ShapeDtypeStruct((528, 128), jnp.bfloat16),
        scratch_shapes=[pltpu.VMEM((NY, 32, 640), jnp.float32)],
        compiler_params=pltpu.CompilerParams(vmem_limit_bytes=4 * 1024 * 1024),
        cost_estimate=pl.CostEstimate(flops=100_000, bytes_accessed=300_000, transcendentals=0),
        name="put",
    )(y, *pieces)


def attend_kernel(q_ref, qr_ref, cos_ref, sin_ref, lat_ref, seg_ref, w_ref, out_ref, key_ref):
    scale = LOG2E / math.sqrt(DN + DR)

    @pl.when(pl.program_id(0) == 0)
    def _():
        low = lax.broadcasted_iota(jnp.int32, (ROWS, 128), 1) < DR
        for j in range(3):
            rows = slice(j * ROWS, (j + 1) * ROWS)
            pair = lat_ref[:, 768 + j * DR : 832 + j * DR]
            tail = jnp.where(low, jnp.concatenate([pair, pair], axis=1), seg_ref[rows])
            for h in range(GROUP):
                key_ref[h, rows, DN:] = tail

    turned = qr_ref[...].astype(jnp.float32)
    lane = lax.broadcasted_iota(jnp.int32, turned.shape, 1)
    first = lane % DR < DR // 2
    swapped = jnp.where(
        first, pltpu.roll(turned, GROUP * DR - DR // 2, 1), pltpu.roll(turned, DR // 2, 1)
    )
    signed = jnp.where(first, -swapped, swapped)
    cosine = jnp.concatenate([cos_ref[...]] * (GROUP // 2), axis=1)
    sine = jnp.concatenate([sin_ref[...]] * (GROUP // 2), axis=1)
    turned = (turned * cosine + signed * sine).astype(jnp.bfloat16)
    row = lax.broadcasted_iota(jnp.int32, (TOK, 64), 0)
    col = lax.broadcasted_iota(jnp.int32, (TOK, 64), 1)
    segment = jnp.where(row // SPAN == col, 1.0, 0.0).astype(jnp.bfloat16)
    ones = jnp.ones((KEYS, 128), jnp.bfloat16)
    r128 = lax.broadcasted_iota(jnp.int32, (128, 128), 0)
    c128 = lax.broadcasted_iota(jnp.int32, (128, 128), 1)
    for h in range(GROUP):
        pair = jnp.concatenate(
            [
                jnp.dot(
                    lat_ref[:, j * 256 : (j + 1) * 256], w_ref[h],
                    preferred_element_type=jnp.float32,
                ).astype(jnp.bfloat16)
                for j in range(3)
            ],
            axis=0,
        )
        query = jnp.concatenate(
            [q_ref[:, h * DN : (h + 1) * DN], turned[:, h * DR : (h + 1) * DR], segment], axis=1
        )
        key_ref[h, :, :DN] = pair[:, :DN]
        scores = lax.dot_general(
            query, key_ref[h], (((1,), (1,)), ((), ())), preferred_element_type=jnp.float32
        )
        highest = jnp.max(scores, axis=1, keepdims=True) * scale
        weights = jnp.exp2(scores * scale - highest).astype(jnp.bfloat16)
        both = jnp.concatenate([pair[:, DN:], ones], axis=1)
        sums = jnp.dot(weights, both, preferred_element_type=jnp.float32)
        norm = sums[:, DV:]
        out_ref[h, :TOK, :] = (sums[:, :DV] / norm).astype(jnp.bfloat16)
        level = highest + jnp.log2(norm)
        upper = jnp.sum(jnp.where(r128 == c128, level[:128], 0.0), axis=0, keepdims=True)
        lower = jnp.sum(
            jnp.where(r128[:64] == c128[:64], level[128:], 0.0), axis=0, keepdims=True
        )
        rest = jnp.concatenate([upper, lower], axis=0)
        rows = []
        for _ in range(3):
            part = rest.astype(jnp.bfloat16).astype(jnp.float32)
            rows.append(part)
            rest = rest - part
        rows.append(jnp.zeros((PAD - TOK - 6, 128), jnp.float32))
        out_ref[h, TOK:, :] = jnp.concatenate(rows, axis=0).astype(jnp.bfloat16)


def attend(query, query_rotary, cosine, sine, lat, seg, weights):
    return pl.pallas_call(
        attend_kernel,
        grid=(H // GROUP,),
        in_specs=[
            pl.BlockSpec((TOK, GROUP * DN), lambda i: (0, i)),
            pl.BlockSpec((TOK, GROUP * DR), lambda i: (0, i)),
            pl.BlockSpec((TOK, 2 * DR), lambda i: (0, 0)),
            pl.BlockSpec((TOK, 2 * DR), lambda i: (0, 0)),
            pl.BlockSpec((ROWS, 960), lambda i: (0, 0)),
            pl.BlockSpec((KEYS, 128), lambda i: (0, 0)),
            pl.BlockSpec((GROUP, 256, 256), lambda i: (i, 0, 0)),
        ],
        out_specs=pl.BlockSpec((GROUP, PAD, 128), lambda i: (i, 0, 0)),
        out_shape=jax.ShapeDtypeStruct((H, PAD, 128), jnp.bfloat16),
        scratch_shapes=[pltpu.VMEM((GROUP, KEYS, 256), jnp.bfloat16)],
        compiler_params=pltpu.CompilerParams(
            dimension_semantics=("arbitrary",), vmem_limit_bytes=24 * 1024 * 1024
        ),
        cost_estimate=pl.CostEstimate(
            flops=3_000_000_000, bytes_accessed=4_000_000, transcendentals=2_400_000
        ),
        name="attend",
    )(query, query_rotary, cosine, sine, lat, seg, weights)


def merge_kernel(in_ref, out_ref):
    levels = []
    for j in range(H):
        tail = in_ref[j, TOK:, :].astype(jnp.float32)
        levels.append(tail[0:2] + tail[2:4] + tail[4:6])
    top = levels[0]
    for level in levels[1:]:
        top = jnp.maximum(top, level)
    factors = [jnp.exp2(level - top) for level in levels]
    total = factors[0]
    for factor in factors[1:]:
        total = total + factor
    r128 = lax.broadcasted_iota(jnp.int32, (128, 128), 0)
    c128 = lax.broadcasted_iota(jnp.int32, (128, 128), 1)
    acc = jnp.zeros((TOK, 128), jnp.float32)
    for j in range(H):
        share = factors[j] / total
        upper = jnp.sum(jnp.where(r128 == c128, share[0:1], 0.0), axis=1, keepdims=True)
        lower = jnp.sum(
            jnp.where(r128[:64] == c128[:64], share[1:2], 0.0), axis=1, keepdims=True
        )
        column = jnp.concatenate([upper, lower], axis=0)
        acc = acc + column * in_ref[j, :TOK, :].astype(jnp.float32)
    merged = acc.astype(jnp.bfloat16)
    for j in range(H):
        out_ref[j] = merged


def merge(parts):
    return pl.pallas_call(
        merge_kernel,
        out_shape=jax.ShapeDtypeStruct((H, TOK, 128), jnp.bfloat16),
        compiler_params=pltpu.CompilerParams(vmem_limit_bytes=8 * 1024 * 1024),
        cost_estimate=pl.CostEstimate(flops=1_000_000, bytes_accessed=500_000, transcendentals=3000),
        name="merge",
    )(parts)


def mix_kernel(rows_ref, gain_ref, w_hbm, out_ref, n_ref, w_ref, sem):
    copies = [
        pltpu.make_async_copy(w_hbm.at[z], w_ref.at[:, pl.ds(z * 128, 128)], sem.at[z])
        for z in range(NZ)
    ]
    for copy in copies:
        copy.start()
    for y in range(NY):
        square = jnp.zeros((HALF, 256), jnp.float32)
        for f in range(H):
            piece = rows_ref[y * H + f].astype(jnp.float32)
            square = square + piece * piece
        factor = lax.rsqrt(jnp.sum(square, axis=1, keepdims=True) / 2048.0 + epsilon)
        for f in range(H):
            piece = rows_ref[y * H + f].astype(jnp.float32)
            n_ref[y * HALF : (y + 1) * HALF, f * 256 : (f + 1) * 256] = (
                piece * factor * gain_ref[:, f * 256 : (f + 1) * 256]
            ).astype(jnp.bfloat16)
    for copy in copies:
        copy.wait()
    dims = (((1,), (1,)), ((), ()))
    hidden = []
    for c in range(NC):
        gate = lax.dot_general(
            n_ref[...], w_ref[c * 528 : c * 528 + 176], dims, preferred_element_type=jnp.float32
        )
        up = lax.dot_general(
            n_ref[...], w_ref[c * 528 + 176 : c * 528 + 352], dims,
            preferred_element_type=jnp.float32,
        )
        hidden.append((gate / (1.0 + jnp.exp(-gate)) * up).astype(jnp.bfloat16))
    for f in range(H):
        lanes = slice(f * 256, (f + 1) * 256)
        part = sum(
            jnp.dot(
                hidden[c], w_ref[c * 528 + 352 : (c + 1) * 528, lanes],
                preferred_element_type=jnp.float32,
            )
            for c in range(NC)
        ).astype(jnp.bfloat16)
        for y in range(NY):
            out_ref[y * H + f] = part[y * HALF : (y + 1) * HALF]


def mix(rows, gain, weights):
    whole = pl.BlockSpec(memory_space=pltpu.VMEM)
    return pl.pallas_call(
        mix_kernel,
        in_specs=[whole, whole, pl.BlockSpec(memory_space=pltpu.HBM)],
        out_specs=whole,
        out_shape=jax.ShapeDtypeStruct((NY * H, HALF, 256), jnp.bfloat16),
        scratch_shapes=[
            pltpu.VMEM((NY * HALF, 2048), jnp.bfloat16),
            pltpu.VMEM((1056, 2048), jnp.bfloat16),
            pltpu.SemaphoreType.DMA((NZ,)),
        ],
        compiler_params=pltpu.CompilerParams(vmem_limit_bytes=52_000_000),
        cost_estimate=pl.CostEstimate(
            flops=1_700_000_000, bytes_accessed=8_000_000, transcendentals=140_000
        ),
        name="mix",
    )(rows, gain, weights)


def project_kernel(heads_ref, w_ref, res_ref, mixed_ref, sent_ref):
    heads = jnp.concatenate([heads_ref[h] for h in range(H)], axis=1)
    mixed = (
        res_ref[...].astype(jnp.float32)
        + jnp.dot(heads, w_ref[...], preferred_element_type=jnp.float32)
    ).astype(jnp.bfloat16)
    mixed_ref[...] = mixed
    for d in range(NY * NX):
        for c in range(NC):
            sent_ref[d * NC + c] = mixed[c * HALF : (c + 1) * HALF]


def project(heads, weights, residual):
    return pl.pallas_call(
        project_kernel,
        out_shape=(
            jax.ShapeDtypeStruct((TOK, 256), jnp.bfloat16),
            jax.ShapeDtypeStruct((NY * NX * NC, HALF, 256), jnp.bfloat16),
        ),
        compiler_params=pltpu.CompilerParams(vmem_limit_bytes=12 * 1024 * 1024),
        cost_estimate=pl.CostEstimate(
            flops=100_000_000, bytes_accessed=3_000_000, transcendentals=0
        ),
        name="project",
    )(heads, weights, residual)


def layer(
    query_content,
    query_rotary,
    latents,
    key_rotary,
    latent_gain,
    key_up,
    value_up,
    out_proj,
    residual,
    mixer_gain,
    gate_proj,
    up_proj,
    down_proj,
):
    zi, yi = lax.axis_index("z"), lax.axis_index("y")
    sp_index = zi * NY + yi
    tp_index = lax.axis_index("x") * NC + lax.axis_index("c")

    own_places = (sp_index * 8 + tp_index) * 24 + jnp.arange(24, dtype=jnp.int32)
    cosine, sine = tables(own_places)
    y_word = yi.reshape(1).astype(jnp.int32)
    own, kv, ahead = prepare(
        y_word, latents, key_rotary, latent_gain.reshape(1, -1), cosine, sine, key_up, value_up,
        gate_proj, up_proj, down_proj.T,
    )
    kv = lax.all_gather(kv, ("x", "c"), axis=0, tiled=False)

    lat = lax.all_to_all(own, "z", split_axis=0, concat_axis=0, tiled=True)
    lat = lat.reshape(NZ * 8, 960)
    pieces = [ahead[s] for s in range(NY)]
    back = [
        lax.ppermute(pieces[s], "y", [(i, (i + s) % NY) for i in range(NY)]) for s in range(1, NY)
    ]
    own_slice = put(y_word, pieces[0], *back)
    mixer = lax.all_gather(own_slice, ("z", "c"), axis=0, tiled=True).reshape(
        NZ, NC * 528, 128
    )

    lat = lax.all_gather(lat, "y", axis=0, tiled=True)

    index = jnp.arange(KEYS, dtype=jnp.int32)
    y_of, z_of, i_of = index // 128 % NY, index // 8 % NZ, index // 512 * 8 + index % 8
    key_segment = (((z_of * NY + y_of) * 8 + tp_index) * 24 + i_of) // SPAN
    ahead_of = (key_segment - sp_index * (TOK // SPAN))[:, None]
    lane = jnp.arange(128, dtype=jnp.int32)[None, :] - DR
    hidden_from = (lane >= 0) & (lane < TOK // SPAN) & (ahead_of > lane)
    seg = jnp.where(hidden_from, masked_score, 0.0).astype(jnp.bfloat16)
    cosine, sine = tables(sp_index * TOK + jnp.arange(TOK, dtype=jnp.int32))
    cosine, sine = (jnp.concatenate([t] * 4, axis=1) for t in (cosine, sine))

    parts = attend(query_content, query_rotary, cosine, sine, lat, seg, kv)
    parts = lax.all_to_all(parts, ("x", "c"), split_axis=0, concat_axis=0, tiled=True)
    heads = lax.all_to_all(merge(parts), ("x", "c"), split_axis=0, concat_axis=0, tiled=True)
    mixed_rows, sent = project(heads, out_proj, residual)
    rows = lax.all_to_all(sent, ("y", "x", "c"), split_axis=0, concat_axis=0, tiled=True)
    partial_sums = mix(rows, mixer_gain.reshape(1, -1), mixer)
    arrived = lax.all_to_all(
        partial_sums, ("y", "x", "c"), split_axis=0, concat_axis=0, tiled=True
    )
    summed = arrived.reshape(NY * NX, TOK, 256).astype(jnp.float32).sum(axis=0)
    return (mixed_rows.astype(jnp.float32) + summed).astype(jnp.bfloat16)


def solution(mesh):
    fine = Mesh(mesh.devices.reshape(NZ, NY, NX, NC), ("z", "y", "x", "c"))
    sp, tp = ("z", "y"), ("x", "c")
    return jax.shard_map(
        layer,
        mesh=fine,
        in_specs=(
            P(sp, None),
            P(sp, None),
            P((*sp, *tp), None),
            P((*sp, *tp), None),
            P(),
            P(None, tp),
            P(None, tp),
            P(None, tp),
            P(sp, tp),
            P(),
            P(sp, tp),
            P(sp, tp),
            P(tp, sp),
        ),
        out_specs=P(sp, tp),
        check_vma=False,
    )
```

```python
import math

import jax
import jax.numpy as jnp
from jax import lax
from jax.experimental import pallas as pl
from jax.experimental.pallas import tpu as pltpu
from jax.sharding import Mesh, PartitionSpec as P


H = 8
DN = 128
DR = 64
DV = 128
SPAN = 64
NZ, NY, NX, NC = 16, 4, 4, 2
NP = 2
TOK = 192
HALF = TOK // 2
KEYS = 1536
PAD = 208
GROUP = 4
ROWS = KEYS // 3

epsilon = 1e-06
masked_score = -1e30
LOG2E = 1.4426950408889634


def tables(places):
    inverse = 10000.0 ** (-jnp.arange(0, DR, 2, dtype=jnp.float32) / DR)
    angles = places.astype(jnp.float32)[:, None] * inverse[None, :]
    return jnp.cos(angles), jnp.sin(angles)


def prepare_kernel(
    word_ref, lat_ref, rot_ref, gain_ref, cos_ref, sin_ref, k_ref, v_ref, gate_ref, up_ref,
    down_ref, out_ref, kv_ref, same_ref, cross_ref,
):
    even = word_ref[0] % NP == 0
    halves = []
    for k in range(NP):
        block = slice(k * 352, (k + 1) * 352)
        halves.append(
            jnp.concatenate([gate_ref[:, block], up_ref[:, block], down_ref[:, block]], axis=1)
        )
    same_ref[...] = jnp.where(even, halves[0], halves[1])
    cross_ref[...] = jnp.where(even, halves[1], halves[0])
    kv_ref[:, :DN] = k_ref[...]
    kv_ref[:, DN:] = v_ref[...]
    widened = lat_ref[...].astype(jnp.float32)
    factor = lax.rsqrt(jnp.mean(widened * widened, axis=-1, keepdims=True) + epsilon)
    normed = (widened * factor * gain_ref[...]).astype(jnp.bfloat16)
    widened = rot_ref[...].astype(jnp.float32)
    a, b = widened[:, : DR // 2], widened[:, DR // 2 :]
    cosine, sine = cos_ref[...], sin_ref[...]
    turned = jnp.concatenate([a * cosine - b * sine, b * cosine + a * sine], axis=-1)
    turned = turned.astype(jnp.bfloat16)
    keys = [slice(j * 8, (j + 1) * 8) for j in range(3)]
    row = jnp.concatenate([normed[k] for k in keys] + [turned[k] for k in keys], axis=1)
    for z in range(NZ):
        out_ref[z] = row


def prepare(*inputs):
    return pl.pallas_call(
        prepare_kernel,
        out_shape=(
            jax.ShapeDtypeStruct((NZ, 8, 960), jnp.bfloat16),
            jax.ShapeDtypeStruct((256, 256), jnp.bfloat16),
            jax.ShapeDtypeStruct((32, 1056), jnp.bfloat16),
            jax.ShapeDtypeStruct((32, 1056), jnp.bfloat16),
        ),
        in_specs=[pl.BlockSpec(memory_space=pltpu.SMEM)]
        + [pl.BlockSpec(memory_space=pltpu.VMEM)] * 10,
        compiler_params=pltpu.CompilerParams(vmem_limit_bytes=66_900_000),
        cost_estimate=pl.CostEstimate(flops=100_000, bytes_accessed=300_000, transcendentals=24),
        name="prepare",
    )(*inputs)


def put_kernel(word_ref, a_ref, b_ref, c_ref, d_ref, out_ref, all_ref):
    y = word_ref[0]
    for s, ref in enumerate((a_ref, b_ref, c_ref, d_ref)):
        all_ref[(y + NY - s) % NY, :, :1056] = ref[...].astype(jnp.float32)
    for k in range(9):
        lanes = jnp.concatenate(
            [all_ref[r, :, k * 128 : (k + 1) * 128] for r in range(NY)], axis=0
        )
        rows = min(128, 1056 - k * 128)
        out_ref[k * 128 : k * 128 + rows] = lanes.T[:rows].astype(jnp.bfloat16)


def put(words, *pieces):
    small = pl.BlockSpec(memory_space=pltpu.VMEM)
    return pl.pallas_call(
        put_kernel,
        in_specs=[pl.BlockSpec(memory_space=pltpu.SMEM), small, small, small, small],
        out_shape=jax.ShapeDtypeStruct((1056, 128), jnp.bfloat16),
        scratch_shapes=[pltpu.VMEM((NY, 32, 1152), jnp.float32)],
        compiler_params=pltpu.CompilerParams(vmem_limit_bytes=6 * 1024 * 1024),
        cost_estimate=pl.CostEstimate(flops=100_000, bytes_accessed=600_000, transcendentals=0),
        name="put",
    )(words, *pieces)


def attend_kernel(
    word_ref, q_ref, qr_ref, cos_ref, sin_ref, lat_ref, seg_ref, w0, w1, w2, w3, out_ref, key_ref
):
    scale = LOG2E / math.sqrt(DN + DR)

    @pl.when(pl.program_id(0) == 0)
    def _():
        low = lax.broadcasted_iota(jnp.int32, (ROWS, 128), 1) < DR
        for j in range(3):
            rows = slice(j * ROWS, (j + 1) * ROWS)
            pair = lat_ref[:, 768 + j * DR : 832 + j * DR]
            tail = jnp.where(low, jnp.concatenate([pair, pair], axis=1), seg_ref[rows])
            for h in range(GROUP):
                key_ref[h, rows, DN:] = tail

    parity = (word_ref[2] + pl.program_id(0)) % NC
    row = lax.broadcasted_iota(jnp.int32, (TOK, 64), 0)
    col = lax.broadcasted_iota(jnp.int32, (TOK, 64), 1)
    segment = jnp.where(row // SPAN == col, 1.0, 0.0).astype(jnp.bfloat16)
    ones = jnp.ones((KEYS, 128), jnp.bfloat16)
    r128 = lax.broadcasted_iota(jnp.int32, (128, 128), 0)
    c128 = lax.broadcasted_iota(jnp.int32, (128, 128), 1)
    lane = lax.broadcasted_iota(jnp.int32, (TOK, 2 * DR), 1)
    first = lane % DR < DR // 2
    for h, w_ref in enumerate((w0, w1, w2, w3)):
        chip = (word_ref[1] + NX - h) % NX
        head = chip * NC + parity
        turned = qr_ref[:, pl.ds(pl.multiple_of(chip * 2 * DR, 128), 2 * DR)].astype(jnp.float32)
        swapped = jnp.where(
            first, pltpu.roll(turned, 2 * DR - DR // 2, 1), pltpu.roll(turned, DR // 2, 1)
        )
        signed = jnp.where(first, -swapped, swapped)
        turned = (turned * cos_ref[...] + signed * sin_ref[...]).astype(jnp.bfloat16)
        turned = jnp.where(parity == 0, turned[:, :DR], turned[:, DR:])
        content = q_ref[:, pl.ds(pl.multiple_of(head * DN, 128), DN)]
        pair = jnp.concatenate(
            [
                jnp.dot(
                    lat_ref[:, j * 256 : (j + 1) * 256], w_ref[0],
                    preferred_element_type=jnp.float32,
                ).astype(jnp.bfloat16)
                for j in range(3)
            ],
            axis=0,
        )
        query = jnp.concatenate([content, turned, segment], axis=1)
        key_ref[h, :, :DN] = pair[:, :DN]
        scores = lax.dot_general(
            query, key_ref[h], (((1,), (1,)), ((), ())), preferred_element_type=jnp.float32
        )
        highest = jnp.max(scores, axis=1, keepdims=True) * scale
        weights = jnp.exp2(scores * scale - highest).astype(jnp.bfloat16)
        both = jnp.concatenate([pair[:, DN:], ones], axis=1)
        sums = jnp.dot(weights, both, preferred_element_type=jnp.float32)
        norm = sums[:, DV:]
        out_ref[head, :TOK, :] = (sums[:, :DV] / norm).astype(jnp.bfloat16)
        level = highest + jnp.log2(norm)
        upper = jnp.sum(jnp.where(r128 == c128, level[:128], 0.0), axis=0, keepdims=True)
        lower = jnp.sum(
            jnp.where(r128[:64] == c128[:64], level[128:], 0.0), axis=0, keepdims=True
        )
        rest = jnp.concatenate([upper, lower], axis=0)
        rows = []
        for _ in range(3):
            part = rest.astype(jnp.bfloat16).astype(jnp.float32)
            rows.append(part)
            rest = rest - part
        rows.append(jnp.zeros((PAD - TOK - 6, 128), jnp.float32))
        out_ref[head, TOK:, :] = jnp.concatenate(rows, axis=0).astype(jnp.bfloat16)


def attend(words, query, query_rotary, cosine, sine, lat, seg, weights):
    def whole(*shape):
        return pl.BlockSpec(shape, lambda i: (0,) * len(shape))

    return pl.pallas_call(
        attend_kernel,
        grid=(NC,),
        in_specs=[
            pl.BlockSpec(memory_space=pltpu.SMEM),
            whole(TOK, H * DN),
            whole(TOK, H * DR),
            whole(TOK, 2 * DR),
            whole(TOK, 2 * DR),
            whole(ROWS, 960),
            whole(KEYS, 128),
        ]
        + [pl.BlockSpec((1, 256, 256), lambda i: (i, 0, 0))] * NX,
        out_specs=whole(H, PAD, 128),
        out_shape=jax.ShapeDtypeStruct((H, PAD, 128), jnp.bfloat16),
        scratch_shapes=[pltpu.VMEM((GROUP, KEYS, 256), jnp.bfloat16)],
        compiler_params=pltpu.CompilerParams(
            dimension_semantics=("arbitrary",), vmem_limit_bytes=24 * 1024 * 1024
        ),
        cost_estimate=pl.CostEstimate(
            flops=3_000_000_000, bytes_accessed=4_000_000, transcendentals=2_400_000
        ),
        name="attend",
    )(words, query, query_rotary, cosine, sine, lat, seg, *weights)


def merge_kernel(in_ref, out_ref):
    levels = []
    for j in range(H):
        tail = in_ref[j, TOK:, :].astype(jnp.float32)
        levels.append(tail[0:2] + tail[2:4] + tail[4:6])
    top = levels[0]
    for level in levels[1:]:
        top = jnp.maximum(top, level)
    factors = [jnp.exp2(level - top) for level in levels]
    total = factors[0]
    for factor in factors[1:]:
        total = total + factor
    r128 = lax.broadcasted_iota(jnp.int32, (128, 128), 0)
    c128 = lax.broadcasted_iota(jnp.int32, (128, 128), 1)
    acc = jnp.zeros((TOK, 128), jnp.float32)
    for j in range(H):
        share = factors[j] / total
        upper = jnp.sum(jnp.where(r128 == c128, share[0:1], 0.0), axis=1, keepdims=True)
        lower = jnp.sum(
            jnp.where(r128[:64] == c128[:64], share[1:2], 0.0), axis=1, keepdims=True
        )
        column = jnp.concatenate([upper, lower], axis=0)
        acc = acc + column * in_ref[j, :TOK, :].astype(jnp.float32)
    merged = acc.astype(jnp.bfloat16)
    for j in range(H):
        out_ref[j] = merged


def merge(parts):
    return pl.pallas_call(
        merge_kernel,
        out_shape=jax.ShapeDtypeStruct((H, TOK, 128), jnp.bfloat16),
        compiler_params=pltpu.CompilerParams(vmem_limit_bytes=8 * 1024 * 1024),
        cost_estimate=pl.CostEstimate(flops=1_000_000, bytes_accessed=500_000, transcendentals=3000),
        name="merge",
    )(parts)


def mix_kernel(rows_ref, gain_ref, w_hbm, out_ref, n_ref, w_ref, sem):
    copies = [
        pltpu.make_async_copy(w_hbm.at[z], w_ref.at[:, pl.ds(z * 128, 128)], sem.at[z])
        for z in range(NZ)
    ]
    for copy in copies:
        copy.start()
    for y in range(NP):
        square = jnp.zeros((HALF, 256), jnp.float32)
        for f in range(H):
            piece = rows_ref[y * H + f].astype(jnp.float32)
            square = square + piece * piece
        factor = lax.rsqrt(jnp.sum(square, axis=1, keepdims=True) / 2048.0 + epsilon)
        for f in range(H):
            piece = rows_ref[y * H + f].astype(jnp.float32)
            n_ref[y * HALF : (y + 1) * HALF, f * 256 : (f + 1) * 256] = (
                piece * factor * gain_ref[:, f * 256 : (f + 1) * 256]
            ).astype(jnp.bfloat16)
    dims = (((1,), (1,)), ((), ()))
    totals = [None] * (2 * NC)
    for chunk in range(4):
        for copy in copies[chunk * 4 : (chunk + 1) * 4]:
            copy.wait()
        lanes = slice(chunk * 512, (chunk + 1) * 512)
        for k in range(2 * NC):
            start = k // 2 * 1056 + k % 2 * 352
            part = lax.dot_general(
                n_ref[:, lanes], w_ref[start : start + 352, lanes], dims,
                preferred_element_type=jnp.float32,
            )
            totals[k] = part if totals[k] is None else totals[k] + part
    hidden = [
        (totals[2 * c] / (1.0 + jnp.exp(-totals[2 * c])) * totals[2 * c + 1]).astype(jnp.bfloat16)
        for c in range(NC)
    ]
    for f in range(H):
        lanes = slice(f * 256, (f + 1) * 256)
        part = sum(
            jnp.dot(
                hidden[c], w_ref[c * 1056 + 704 : (c + 1) * 1056, lanes],
                preferred_element_type=jnp.float32,
            )
            for c in range(NC)
        ).astype(jnp.bfloat16)
        for y in range(NP):
            out_ref[y * H + f] = part[y * HALF : (y + 1) * HALF]


def mix(rows, gain, weights):
    whole = pl.BlockSpec(memory_space=pltpu.VMEM)
    return pl.pallas_call(
        mix_kernel,
        in_specs=[whole, whole, pl.BlockSpec(memory_space=pltpu.HBM)],
        out_specs=whole,
        out_shape=jax.ShapeDtypeStruct((NP * H, HALF, 256), jnp.bfloat16),
        scratch_shapes=[
            pltpu.VMEM((NP * HALF, 2048), jnp.bfloat16),
            pltpu.VMEM((NC * 1056, 2048), jnp.bfloat16),
            pltpu.SemaphoreType.DMA((NZ,)),
        ],
        compiler_params=pltpu.CompilerParams(vmem_limit_bytes=52_000_000),
        cost_estimate=pl.CostEstimate(
            flops=1_700_000_000, bytes_accessed=10_000_000, transcendentals=140_000
        ),
        name="mix",
    )(rows, gain, weights)


def project_kernel(heads_ref, w_ref, res_ref, mixed_ref, sent_ref):
    heads = jnp.concatenate([heads_ref[h] for h in range(H)], axis=1)
    mixed = (
        res_ref[...].astype(jnp.float32)
        + jnp.dot(heads, w_ref[...], preferred_element_type=jnp.float32)
    ).astype(jnp.bfloat16)
    mixed_ref[...] = mixed
    for d in range(NP * NX):
        for c in range(NC):
            sent_ref[d * NC + c] = mixed[c * HALF : (c + 1) * HALF]


def project(heads, weights, residual):
    return pl.pallas_call(
        project_kernel,
        out_shape=(
            jax.ShapeDtypeStruct((TOK, 256), jnp.bfloat16),
            jax.ShapeDtypeStruct((NP * NX * NC, HALF, 256), jnp.bfloat16),
        ),
        compiler_params=pltpu.CompilerParams(vmem_limit_bytes=12 * 1024 * 1024),
        cost_estimate=pl.CostEstimate(
            flops=100_000_000, bytes_accessed=3_000_000, transcendentals=0
        ),
        name="project",
    )(heads, weights, residual)


def layer(
    query_content,
    query_rotary,
    latents,
    key_rotary,
    latent_gain,
    key_up,
    value_up,
    out_proj,
    residual,
    mixer_gain,
    gate_proj,
    up_proj,
    down_proj,
):
    zi, yi = lax.axis_index("z"), lax.axis_index("g") * NP + lax.axis_index("p")
    sp_index = zi * NY + yi
    tp_index = lax.axis_index("x") * NC + lax.axis_index("c")

    own_places = (sp_index * 8 + tp_index) * 24 + jnp.arange(24, dtype=jnp.int32)
    cosine, sine = tables(own_places)
    words = jnp.stack([yi, lax.axis_index("x"), lax.axis_index("c")]).astype(jnp.int32)
    own, kv, same, cross = prepare(
        words, latents, key_rotary, latent_gain.reshape(1, -1), cosine, sine, key_up, value_up,
        gate_proj, up_proj, down_proj.T,
    )
    back = [same] + [
        lax.ppermute(piece, ("g", "p"), [(i, (i + s) % NY) for i in range(NY)])
        for s, piece in ((1, cross), (2, same), (3, cross))
    ]
    mixer = lax.all_gather(put(words, *back), ("z", "c"), axis=0, tiled=True)
    mixer = mixer.reshape(NZ, NC * 1056, 128)

    lat = lax.all_to_all(own, "z", split_axis=0, concat_axis=0, tiled=True)
    lat = lat.reshape(NZ * 8, 960)
    pair = jnp.stack([kv, lax.ppermute(kv, "c", [(0, 1), (1, 0)])])
    weights = [pair] + [
        lax.ppermute(pair, "x", [(i, (i + s) % NX) for i in range(NX)]) for s in range(1, NX)
    ]

    lat = lax.all_gather(lat, ("g", "p"), axis=0, tiled=True)

    index = jnp.arange(KEYS, dtype=jnp.int32)
    y_of, z_of, i_of = index // 128 % NY, index // 8 % NZ, index // 512 * 8 + index % 8
    key_segment = (((z_of * NY + y_of) * 8 + tp_index) * 24 + i_of) // SPAN
    ahead_of = (key_segment - sp_index * (TOK // SPAN))[:, None]
    lane = jnp.arange(128, dtype=jnp.int32)[None, :] - DR
    hidden_from = (lane >= 0) & (lane < TOK // SPAN) & (ahead_of > lane)
    seg = jnp.where(hidden_from, masked_score, 0.0).astype(jnp.bfloat16)
    cosine, sine = tables(sp_index * TOK + jnp.arange(TOK, dtype=jnp.int32))
    cosine, sine = (jnp.concatenate([t] * 4, axis=1) for t in (cosine, sine))

    parts = attend(words, query_content, query_rotary, cosine, sine, lat, seg, weights)
    parts = lax.all_to_all(parts, ("x", "c"), split_axis=0, concat_axis=0, tiled=True)
    heads = lax.all_to_all(merge(parts), ("x", "c"), split_axis=0, concat_axis=0, tiled=True)
    mixed_rows, sent = project(heads, out_proj, residual)
    rows = lax.all_to_all(sent, ("p", "x", "c"), split_axis=0, concat_axis=0, tiled=True)
    partial_sums = mix(rows, mixer_gain.reshape(1, -1), mixer)
    arrived = lax.all_to_all(
        partial_sums, ("p", "x", "c"), split_axis=0, concat_axis=0, tiled=True
    )
    summed = arrived.reshape(NP * NX, TOK, 256).astype(jnp.float32).sum(axis=0)
    return (mixed_rows.astype(jnp.float32) + summed).astype(jnp.bfloat16)


def solution(mesh):
    fine = Mesh(mesh.devices.reshape(NZ, NY // NP, NP, NX, NC), ("z", "g", "p", "x", "c"))
    sp, tp = ("z", "g", "p"), ("x", "c")
    return jax.shard_map(
        layer,
        mesh=fine,
        in_specs=(
            P(sp, None),
            P(sp, None),
            P((*sp, *tp), None),
            P((*sp, *tp), None),
            P(),
            P(None, tp),
            P(None, tp),
            P(None, tp),
            P(sp, tp),
            P(),
            P(sp, tp),
            P(sp, tp),
            P(tp, sp),
        ),
        out_specs=P(sp, tp),
        check_vma=False,
    )
```

```python
import math

import jax
import jax.numpy as jnp
from jax import lax
from jax.experimental import pallas as pl
from jax.experimental.pallas import tpu as pltpu
from jax.sharding import Mesh, PartitionSpec as P


H = 8
DN = 128
DR = 64
DV = 128
SPAN = 64
NZ, NY, NX, NC = 16, 4, 4, 2
NP = 2
TOK = 192
HALF = TOK // 2
KEYS = 1536
PAD = 208
GROUP = 4
ROWS = KEYS // 3

epsilon = 1e-06
masked_score = -1e30
LOG2E = 1.4426950408889634


def tables(places):
    inverse = 10000.0 ** (-jnp.arange(0, DR, 2, dtype=jnp.float32) / DR)
    angles = places.astype(jnp.float32)[:, None] * inverse[None, :]
    return jnp.cos(angles), jnp.sin(angles)


def prepare_kernel(
    lat_ref, rot_ref, gain_ref, cos_ref, sin_ref, k_ref, v_ref, gate_ref, up_ref, down_ref,
    out_ref, kv_ref, cut_ref,
):
    for k in range(NP):
        block = slice(k * 352, (k + 1) * 352)
        half = jnp.concatenate(
            [gate_ref[:, block], up_ref[:, block], down_ref[:, block]], axis=1
        )
        for y in range(k, NY, NP):
            cut_ref[y] = half
    kv_ref[:, :DN] = k_ref[...]
    kv_ref[:, DN:] = v_ref[...]
    widened = lat_ref[...].astype(jnp.float32)
    factor = lax.rsqrt(jnp.mean(widened * widened, axis=-1, keepdims=True) + epsilon)
    normed = (widened * factor * gain_ref[...]).astype(jnp.bfloat16)
    widened = rot_ref[...].astype(jnp.float32)
    a, b = widened[:, : DR // 2], widened[:, DR // 2 :]
    cosine, sine = cos_ref[...], sin_ref[...]
    turned = jnp.concatenate([a * cosine - b * sine, b * cosine + a * sine], axis=-1)
    turned = turned.astype(jnp.bfloat16)
    keys = [slice(j * 8, (j + 1) * 8) for j in range(3)]
    row = jnp.concatenate([normed[k] for k in keys] + [turned[k] for k in keys], axis=1)
    for z in range(NZ):
        out_ref[z] = row


def prepare(*inputs):
    return pl.pallas_call(
        prepare_kernel,
        out_shape=(
            jax.ShapeDtypeStruct((NZ, 8, 960), jnp.bfloat16),
            jax.ShapeDtypeStruct((256, 256), jnp.bfloat16),
            jax.ShapeDtypeStruct((NY, 32, 1056), jnp.bfloat16),
        ),
        compiler_params=pltpu.CompilerParams(vmem_limit_bytes=66_900_000),
        cost_estimate=pl.CostEstimate(flops=100_000, bytes_accessed=300_000, transcendentals=24),
        name="prepare",
    )(*inputs)


def put_kernel(in_ref, out_ref, all_ref):
    for r in range(NY):
        all_ref[r, :, :1056] = in_ref[r].astype(jnp.float32)
    for k in range(9):
        lanes = jnp.concatenate(
            [all_ref[r, :, k * 128 : (k + 1) * 128] for r in range(NY)], axis=0
        )
        rows = min(128, 1056 - k * 128)
        out_ref[k * 128 : k * 128 + rows] = lanes.T[:rows].astype(jnp.bfloat16)


def put(pieces):
    return pl.pallas_call(
        put_kernel,
        out_shape=jax.ShapeDtypeStruct((1056, 128), jnp.bfloat16),
        scratch_shapes=[pltpu.VMEM((NY, 32, 1152), jnp.float32)],
        compiler_params=pltpu.CompilerParams(vmem_limit_bytes=6 * 1024 * 1024),
        cost_estimate=pl.CostEstimate(flops=100_000, bytes_accessed=600_000, transcendentals=0),
        name="put",
    )(pieces)


def turn_kernel(q_ref, qr_ref, cos_ref, sin_ref, out_ref):
    lane = lax.broadcasted_iota(jnp.int32, (TOK, 2 * DR), 1)
    first = lane % DR < DR // 2
    row = lax.broadcasted_iota(jnp.int32, (TOK, 64), 0)
    col = lax.broadcasted_iota(jnp.int32, (TOK, 64), 1)
    segment = jnp.where(row // SPAN == col, 1.0, 0.0).astype(jnp.bfloat16)
    for pair in range(H // 2):
        turned = qr_ref[:, pair * 2 * DR : (pair + 1) * 2 * DR].astype(jnp.float32)
        swapped = jnp.where(
            first, pltpu.roll(turned, 2 * DR - DR // 2, 1), pltpu.roll(turned, DR // 2, 1)
        )
        signed = jnp.where(first, -swapped, swapped)
        turned = (turned * cos_ref[...] + signed * sin_ref[...]).astype(jnp.bfloat16)
        for k in range(2):
            h = pair * 2 + k
            out_ref[h, :, :DN] = q_ref[:, h * DN : (h + 1) * DN]
            out_ref[h, :, DN:] = jnp.concatenate(
                [turned[:, k * DR : (k + 1) * DR], segment], axis=1
            )


def turn(*inputs):
    return pl.pallas_call(
        turn_kernel,
        out_shape=jax.ShapeDtypeStruct((H, TOK, 256), jnp.bfloat16),
        compiler_params=pltpu.CompilerParams(vmem_limit_bytes=8 * 1024 * 1024),
        cost_estimate=pl.CostEstimate(flops=500_000, bytes_accessed=1_500_000, transcendentals=0),
        name="turn",
    )(*inputs)


def attend_kernel(
    q_ref, lat_ref, seg_ref, w0, w1, w2, w3, out_ref, key_ref
):
    scale = LOG2E / math.sqrt(DN + DR)

    @pl.when(pl.program_id(0) == 0)
    def _():
        low = lax.broadcasted_iota(jnp.int32, (ROWS, 128), 1) < DR
        for j in range(3):
            rows = slice(j * ROWS, (j + 1) * ROWS)
            pair = lat_ref[:, 768 + j * DR : 832 + j * DR]
            tail = jnp.where(low, jnp.concatenate([pair, pair], axis=1), seg_ref[rows])
            for h in range(GROUP):
                key_ref[h, rows, DN:] = tail

    parity = (lax.axis_index("c") + pl.program_id(0)) % NC
    ones = jnp.ones((KEYS, 128), jnp.bfloat16)
    r128 = lax.broadcasted_iota(jnp.int32, (128, 128), 0)
    c128 = lax.broadcasted_iota(jnp.int32, (128, 128), 1)
    for h, w_ref in enumerate((w0, w1, w2, w3)):
        chip = (lax.axis_index("x") + NX - h) % NX
        head = chip * NC + parity
        pair = jnp.concatenate(
            [
                jnp.dot(
                    lat_ref[:, j * 256 : (j + 1) * 256], w_ref[0],
                    preferred_element_type=jnp.float32,
                ).astype(jnp.bfloat16)
                for j in range(3)
            ],
            axis=0,
        )
        key_ref[h, :, :DN] = pair[:, :DN]
        scores = lax.dot_general(
            q_ref[head], key_ref[h], (((1,), (1,)), ((), ())), preferred_element_type=jnp.float32
        )
        highest = jnp.max(scores, axis=1, keepdims=True) * scale
        weights = jnp.exp2(scores * scale - highest).astype(jnp.bfloat16)
        both = jnp.concatenate([pair[:, DN:], ones], axis=1)
        sums = jnp.dot(weights, both, preferred_element_type=jnp.float32)
        norm = sums[:, DV:]
        out_ref[head, :TOK, :] = (sums[:, :DV] / norm).astype(jnp.bfloat16)
        level = highest + jnp.log2(norm)
        upper = jnp.sum(jnp.where(r128 == c128, level[:128], 0.0), axis=0, keepdims=True)
        lower = jnp.sum(
            jnp.where(r128[:64] == c128[:64], level[128:], 0.0), axis=0, keepdims=True
        )
        rest = jnp.concatenate([upper, lower], axis=0)
        rows = []
        for _ in range(3):
            part = rest.astype(jnp.bfloat16).astype(jnp.float32)
            rows.append(part)
            rest = rest - part
        rows.append(jnp.zeros((PAD - TOK - 6, 128), jnp.float32))
        out_ref[head, TOK:, :] = jnp.concatenate(rows, axis=0).astype(jnp.bfloat16)


def attend(query, lat, seg, weights):
    def whole(*shape):
        return pl.BlockSpec(shape, lambda i: (0,) * len(shape))

    return pl.pallas_call(
        attend_kernel,
        grid=(NC,),
        in_specs=[
            whole(H, TOK, 256),
            whole(ROWS, 960),
            whole(KEYS, 128),
        ]
        + [pl.BlockSpec((1, 256, 256), lambda i: (i, 0, 0))] * NX,
        out_specs=whole(H, PAD, 128),
        out_shape=jax.ShapeDtypeStruct((H, PAD, 128), jnp.bfloat16),
        scratch_shapes=[pltpu.VMEM((GROUP, KEYS, 256), jnp.bfloat16)],
        compiler_params=pltpu.CompilerParams(
            dimension_semantics=("arbitrary",), vmem_limit_bytes=24 * 1024 * 1024
        ),
        cost_estimate=pl.CostEstimate(
            flops=3_000_000_000, bytes_accessed=4_000_000, transcendentals=2_400_000
        ),
        name="attend",
    )(query, lat, seg, *weights)


def merge_kernel(in_ref, out_ref):
    levels = []
    for j in range(H):
        tail = in_ref[j, TOK:, :].astype(jnp.float32)
        levels.append(tail[0:2] + tail[2:4] + tail[4:6])
    top = levels[0]
    for level in levels[1:]:
        top = jnp.maximum(top, level)
    factors = [jnp.exp2(level - top) for level in levels]
    total = factors[0]
    for factor in factors[1:]:
        total = total + factor
    r128 = lax.broadcasted_iota(jnp.int32, (128, 128), 0)
    c128 = lax.broadcasted_iota(jnp.int32, (128, 128), 1)
    acc = jnp.zeros((TOK, 128), jnp.float32)
    for j in range(H):
        share = factors[j] / total
        upper = jnp.sum(jnp.where(r128 == c128, share[0:1], 0.0), axis=1, keepdims=True)
        lower = jnp.sum(
            jnp.where(r128[:64] == c128[:64], share[1:2], 0.0), axis=1, keepdims=True
        )
        column = jnp.concatenate([upper, lower], axis=0)
        acc = acc + column * in_ref[j, :TOK, :].astype(jnp.float32)
    merged = acc.astype(jnp.bfloat16)
    for j in range(H):
        out_ref[j] = merged


def merge(parts):
    return pl.pallas_call(
        merge_kernel,
        out_shape=jax.ShapeDtypeStruct((H, TOK, 128), jnp.bfloat16),
        compiler_params=pltpu.CompilerParams(vmem_limit_bytes=8 * 1024 * 1024),
        cost_estimate=pl.CostEstimate(flops=1_000_000, bytes_accessed=500_000, transcendentals=3000),
        name="merge",
    )(parts)


def mix_kernel(rows_ref, gain_ref, w_hbm, out_ref, n_ref, w_ref, sem):
    copies = [
        pltpu.make_async_copy(w_hbm.at[z], w_ref.at[:, pl.ds(z * 128, 128)], sem.at[z])
        for z in range(NZ)
    ]
    for copy in copies:
        copy.start()
    for y in range(NP):
        square = jnp.zeros((HALF, 256), jnp.float32)
        for f in range(H):
            piece = rows_ref[y * H + f].astype(jnp.float32)
            square = square + piece * piece
        factor = lax.rsqrt(jnp.sum(square, axis=1, keepdims=True) / 2048.0 + epsilon)
        for f in range(H):
            piece = rows_ref[y * H + f].astype(jnp.float32)
            n_ref[y * HALF : (y + 1) * HALF, f * 256 : (f + 1) * 256] = (
                piece * factor * gain_ref[:, f * 256 : (f + 1) * 256]
            ).astype(jnp.bfloat16)
    dims = (((1,), (1,)), ((), ()))
    totals = [None] * (2 * NC)
    for chunk in range(4):
        for copy in copies[chunk * 4 : (chunk + 1) * 4]:
            copy.wait()
        lanes = slice(chunk * 512, (chunk + 1) * 512)
        for k in range(2 * NC):
            start = k // 2 * 1056 + k % 2 * 352
            part = lax.dot_general(
                n_ref[:, lanes], w_ref[start : start + 352, lanes], dims,
                preferred_element_type=jnp.float32,
            )
            totals[k] = part if totals[k] is None else totals[k] + part
    hidden = [
        (totals[2 * c] / (1.0 + jnp.exp(-totals[2 * c])) * totals[2 * c + 1]).astype(jnp.bfloat16)
        for c in range(NC)
    ]
    for f in range(H):
        lanes = slice(f * 256, (f + 1) * 256)
        part = sum(
            jnp.dot(
                hidden[c], w_ref[c * 1056 + 704 : (c + 1) * 1056, lanes],
                preferred_element_type=jnp.float32,
            )
            for c in range(NC)
        ).astype(jnp.bfloat16)
        for y in range(NP):
            out_ref[y * H + f] = part[y * HALF : (y + 1) * HALF]


def mix(rows, gain, weights):
    whole = pl.BlockSpec(memory_space=pltpu.VMEM)
    return pl.pallas_call(
        mix_kernel,
        in_specs=[whole, whole, pl.BlockSpec(memory_space=pltpu.HBM)],
        out_specs=whole,
        out_shape=jax.ShapeDtypeStruct((NP * H, HALF, 256), jnp.bfloat16),
        scratch_shapes=[
            pltpu.VMEM((NP * HALF, 2048), jnp.bfloat16),
            pltpu.VMEM((NC * 1056, 2048), jnp.bfloat16),
            pltpu.SemaphoreType.DMA((NZ,)),
        ],
        compiler_params=pltpu.CompilerParams(vmem_limit_bytes=52_000_000),
        cost_estimate=pl.CostEstimate(
            flops=1_700_000_000, bytes_accessed=10_000_000, transcendentals=140_000
        ),
        name="mix",
    )(rows, gain, weights)


def project_kernel(heads_ref, w_ref, res_ref, mixed_ref, sent_ref):
    heads = jnp.concatenate([heads_ref[h] for h in range(H)], axis=1)
    mixed = (
        res_ref[...].astype(jnp.float32)
        + jnp.dot(heads, w_ref[...], preferred_element_type=jnp.float32)
    ).astype(jnp.bfloat16)
    mixed_ref[...] = mixed
    for d in range(NP * NX):
        for c in range(NC):
            sent_ref[d * NC + c] = mixed[c * HALF : (c + 1) * HALF]


def project(heads, weights, residual):
    return pl.pallas_call(
        project_kernel,
        out_shape=(
            jax.ShapeDtypeStruct((TOK, 256), jnp.bfloat16),
            jax.ShapeDtypeStruct((NP * NX * NC, HALF, 256), jnp.bfloat16),
        ),
        compiler_params=pltpu.CompilerParams(vmem_limit_bytes=12 * 1024 * 1024),
        cost_estimate=pl.CostEstimate(
            flops=100_000_000, bytes_accessed=3_000_000, transcendentals=0
        ),
        name="project",
    )(heads, weights, residual)


def layer(
    query_content,
    query_rotary,
    latents,
    key_rotary,
    latent_gain,
    key_up,
    value_up,
    out_proj,
    residual,
    mixer_gain,
    gate_proj,
    up_proj,
    down_proj,
):
    zi, yi = lax.axis_index("z"), lax.axis_index("g") * NP + lax.axis_index("p")
    sp_index = zi * NY + yi
    tp_index = lax.axis_index("x") * NC + lax.axis_index("c")

    own_places = (sp_index * 8 + tp_index) * 24 + jnp.arange(24, dtype=jnp.int32)
    cosine, sine = tables(own_places)
    own, kv, cut = prepare(
        latents, key_rotary, latent_gain.reshape(1, -1), cosine, sine, key_up, value_up,
        gate_proj, up_proj, down_proj.T,
    )
    cut = lax.all_to_all(cut, ("g", "p"), split_axis=0, concat_axis=0, tiled=True)
    mixer = lax.all_gather(put(cut), ("z", "c"), axis=0, tiled=True)
    mixer = mixer.reshape(NZ, NC * 1056, 128)

    lat = lax.all_to_all(own, "z", split_axis=0, concat_axis=0, tiled=True)
    lat = lat.reshape(NZ * 8, 960)
    partner = lax.ppermute(kv, "c", [(0, 1), (1, 0)])
    pair = jnp.stack([kv, partner])
    weights = [pair] + [
        lax.ppermute(pair, "x", [(i, (i + s) % NX) for i in range(NX)]) for s in range(1, NX)
    ]

    lat = lax.all_gather(lat, ("g", "p"), axis=0, tiled=True)

    index = jnp.arange(KEYS, dtype=jnp.int32)
    y_of, z_of, i_of = index // 128 % NY, index // 8 % NZ, index // 512 * 8 + index % 8
    key_segment = (((z_of * NY + y_of) * 8 + tp_index) * 24 + i_of) // SPAN
    ahead_of = (key_segment - sp_index * (TOK // SPAN))[:, None]
    lane = jnp.arange(128, dtype=jnp.int32)[None, :] - DR
    hidden_from = (lane >= 0) & (lane < TOK // SPAN) & (ahead_of > lane)
    seg = jnp.where(hidden_from, masked_score, 0.0).astype(jnp.bfloat16)
    cosine, sine = tables(sp_index * TOK + jnp.arange(TOK, dtype=jnp.int32))
    cosine, sine = (jnp.concatenate([t] * 4, axis=1) for t in (cosine, sine))

    query = turn(query_content, query_rotary, cosine, sine)
    parts = attend(query, lat, seg, weights)
    parts = lax.all_to_all(parts, ("x", "c"), split_axis=0, concat_axis=0, tiled=True)
    heads = lax.all_to_all(merge(parts), ("x", "c"), split_axis=0, concat_axis=0, tiled=True)
    mixed_rows, sent = project(heads, out_proj, residual)
    rows = lax.all_to_all(sent, ("p", "x", "c"), split_axis=0, concat_axis=0, tiled=True)
    partial_sums = mix(rows, mixer_gain.reshape(1, -1), mixer)
    arrived = lax.all_to_all(
        partial_sums, ("p", "x", "c"), split_axis=0, concat_axis=0, tiled=True
    )
    summed = arrived.reshape(NP * NX, TOK, 256).astype(jnp.float32).sum(axis=0)
    return (mixed_rows.astype(jnp.float32) + summed).astype(jnp.bfloat16)


def solution(mesh):
    fine = Mesh(mesh.devices.reshape(NZ, NY // NP, NP, NX, NC), ("z", "g", "p", "x", "c"))
    sp, tp = ("z", "g", "p"), ("x", "c")
    return jax.shard_map(
        layer,
        mesh=fine,
        in_specs=(
            P(sp, None),
            P(sp, None),
            P((*sp, *tp), None),
            P((*sp, *tp), None),
            P(),
            P(None, tp),
            P(None, tp),
            P(None, tp),
            P(sp, tp),
            P(),
            P(sp, tp),
            P(sp, tp),
            P(tp, sp),
        ),
        out_specs=P(sp, tp),
        check_vma=False,
    )
```

```python
import math

import jax
import jax.numpy as jnp
import numpy as np
from jax import lax
from jax.experimental import pallas as pl
from jax.experimental.pallas import tpu as pltpu
from jax.sharding import Mesh, PartitionSpec as P


H = 8
DN = 128
DR = 64
DV = 128
SPAN = 64
NZ, NY, NX, NC = 16, 4, 4, 2
NP = 2
TOK = 192
HALF = TOK // 2
KEYS = 1536
PAD = 208
GROUP = 4
ROWS = KEYS // 3

epsilon = 1e-06
masked_score = -1e30
LOG2E = 1.4426950408889634


def tables(places):
    inverse = 10000.0 ** (-np.arange(0, DR, 2) / DR)
    angles = np.tile(places[:, None] * inverse[None, :], (1, 4))
    return jnp.asarray(np.concatenate([np.cos(angles), np.sin(angles)], axis=1), jnp.float32)


def joined(block, inside):
    cos_a, sin_a, cos_b, sin_b = block[:, :128], block[:, 128:], inside[:, :128], inside[:, 128:]
    return cos_a * cos_b - sin_a * sin_b, sin_a * cos_b + cos_a * sin_b


def block_index():
    return lax.axis_index("z") * NY + lax.axis_index("g") * NP + lax.axis_index("p")


def prepare_kernel(
    lat_ref, rot_ref, gain_ref, block_ref, inside_ref, k_ref, v_ref, gate_ref, up_ref, down_ref,
    out_ref, kv_ref, cut_ref,
):
    for k in range(NP):
        block = slice(k * 352, (k + 1) * 352)
        half = jnp.concatenate(
            [gate_ref[:, block], up_ref[:, block], down_ref[:, block]], axis=1
        )
        for y in range(k, NY, NP):
            cut_ref[y] = half
    kv_ref[:, :DN] = k_ref[...]
    kv_ref[:, DN:] = v_ref[...]
    widened = lat_ref[...].astype(jnp.float32)
    factor = lax.rsqrt(jnp.mean(widened * widened, axis=-1, keepdims=True) + epsilon)
    normed = (widened * factor * gain_ref[...]).astype(jnp.bfloat16)
    widened = rot_ref[...].astype(jnp.float32)
    a, b = widened[:, : DR // 2], widened[:, DR // 2 :]
    tp = lax.axis_index("x") * NC + lax.axis_index("c")
    cosine, sine = joined(
        block_ref[pl.ds(block_index(), 1), :],
        inside_ref[pl.ds(pl.multiple_of(tp * 24, 8), 24), :],
    )
    cosine, sine = cosine[:, : DR // 2], sine[:, : DR // 2]
    turned = jnp.concatenate([a * cosine - b * sine, b * cosine + a * sine], axis=-1)
    turned = turned.astype(jnp.bfloat16)
    keys = [slice(j * 8, (j + 1) * 8) for j in range(3)]
    row = jnp.concatenate([normed[k] for k in keys] + [turned[k] for k in keys], axis=1)
    for z in range(NZ):
        out_ref[z] = row


def prepare(*inputs):
    return pl.pallas_call(
        prepare_kernel,
        out_shape=(
            jax.ShapeDtypeStruct((NZ, 8, 960), jnp.bfloat16),
            jax.ShapeDtypeStruct((256, 256), jnp.bfloat16),
            jax.ShapeDtypeStruct((NY, 32, 1056), jnp.bfloat16),
        ),
        compiler_params=pltpu.CompilerParams(vmem_limit_bytes=66_900_000),
        cost_estimate=pl.CostEstimate(flops=100_000, bytes_accessed=300_000, transcendentals=24),
        name="prepare",
    )(*inputs)


def put_kernel(in_ref, out_ref, all_ref):
    for r in range(NY):
        all_ref[r, :, :1056] = in_ref[r].astype(jnp.float32)
    for k in range(9):
        lanes = jnp.concatenate(
            [all_ref[r, :, k * 128 : (k + 1) * 128] for r in range(NY)], axis=0
        )
        rows = min(128, 1056 - k * 128)
        out_ref[k * 128 : k * 128 + rows] = lanes.T[:rows].astype(jnp.bfloat16)


def put(pieces):
    return pl.pallas_call(
        put_kernel,
        out_shape=jax.ShapeDtypeStruct((1056, 128), jnp.bfloat16),
        scratch_shapes=[pltpu.VMEM((NY, 32, 1152), jnp.float32)],
        compiler_params=pltpu.CompilerParams(vmem_limit_bytes=6 * 1024 * 1024),
        cost_estimate=pl.CostEstimate(flops=100_000, bytes_accessed=600_000, transcendentals=0),
        name="put",
    )(pieces)


def turn_kernel(q_ref, qr_ref, block_ref, inside_ref, out_ref):
    cosine, sine = joined(block_ref[pl.ds(block_index(), 1), :], inside_ref[...])
    lane = lax.broadcasted_iota(jnp.int32, (TOK, 2 * DR), 1)
    first = lane % DR < DR // 2
    row = lax.broadcasted_iota(jnp.int32, (TOK, 64), 0)
    col = lax.broadcasted_iota(jnp.int32, (TOK, 64), 1)
    segment = jnp.where(row // SPAN == col, 1.0, 0.0).astype(jnp.bfloat16)
    for pair in range(H // 2):
        turned = qr_ref[:, pair * 2 * DR : (pair + 1) * 2 * DR].astype(jnp.float32)
        swapped = jnp.where(
            first, pltpu.roll(turned, 2 * DR - DR // 2, 1), pltpu.roll(turned, DR // 2, 1)
        )
        signed = jnp.where(first, -swapped, swapped)
        turned = (turned * cosine + signed * sine).astype(jnp.bfloat16)
        for k in range(2):
            h = pair * 2 + k
            out_ref[h, :, :DN] = q_ref[:, h * DN : (h + 1) * DN]
            out_ref[h, :, DN:] = jnp.concatenate(
                [turned[:, k * DR : (k + 1) * DR], segment], axis=1
            )


def turn(*inputs):
    return pl.pallas_call(
        turn_kernel,
        out_shape=jax.ShapeDtypeStruct((H, TOK, 256), jnp.bfloat16),
        compiler_params=pltpu.CompilerParams(vmem_limit_bytes=8 * 1024 * 1024),
        cost_estimate=pl.CostEstimate(flops=500_000, bytes_accessed=1_500_000, transcendentals=0),
        name="turn",
    )(*inputs)


def attend_kernel(
    q_ref, lat_ref, seg_ref, w0, w1, w2, w3, out_ref, key_ref
):
    scale = LOG2E / math.sqrt(DN + DR)

    @pl.when(pl.program_id(0) == 0)
    def _():
        low = lax.broadcasted_iota(jnp.int32, (ROWS, 128), 1) < DR
        for j in range(3):
            rows = slice(j * ROWS, (j + 1) * ROWS)
            pair = lat_ref[:, 768 + j * DR : 832 + j * DR]
            tail = jnp.where(low, jnp.concatenate([pair, pair], axis=1), seg_ref[rows])
            for h in range(GROUP):
                key_ref[h, rows, DN:] = tail

    parity = (lax.axis_index("c") + pl.program_id(0)) % NC
    ones = jnp.ones((KEYS, 128), jnp.bfloat16)
    r128 = lax.broadcasted_iota(jnp.int32, (128, 128), 0)
    c128 = lax.broadcasted_iota(jnp.int32, (128, 128), 1)
    for h, w_ref in enumerate((w0, w1, w2, w3)):
        chip = (lax.axis_index("x") + NX - h) % NX
        head = chip * NC + parity
        pair = jnp.concatenate(
            [
                jnp.dot(
                    lat_ref[:, j * 256 : (j + 1) * 256], w_ref[0],
                    preferred_element_type=jnp.float32,
                ).astype(jnp.bfloat16)
                for j in range(3)
            ],
            axis=0,
        )
        key_ref[h, :, :DN] = pair[:, :DN]
        scores = lax.dot_general(
            q_ref[head], key_ref[h], (((1,), (1,)), ((), ())), preferred_element_type=jnp.float32
        )
        highest = jnp.max(scores, axis=1, keepdims=True) * scale
        weights = jnp.exp2(scores * scale - highest).astype(jnp.bfloat16)
        both = jnp.concatenate([pair[:, DN:], ones], axis=1)
        sums = jnp.dot(weights, both, preferred_element_type=jnp.float32)
        norm = sums[:, DV:]
        out_ref[head, :TOK, :] = (sums[:, :DV] / norm).astype(jnp.bfloat16)
        level = highest + jnp.log2(norm)
        upper = jnp.sum(jnp.where(r128 == c128, level[:128], 0.0), axis=0, keepdims=True)
        lower = jnp.sum(
            jnp.where(r128[:64] == c128[:64], level[128:], 0.0), axis=0, keepdims=True
        )
        rest = jnp.concatenate([upper, lower], axis=0)
        rows = []
        for _ in range(3):
            part = rest.astype(jnp.bfloat16).astype(jnp.float32)
            rows.append(part)
            rest = rest - part
        rows.append(jnp.zeros((PAD - TOK - 6, 128), jnp.float32))
        out_ref[head, TOK:, :] = jnp.concatenate(rows, axis=0).astype(jnp.bfloat16)


def attend(query, lat, seg, weights):
    def whole(*shape):
        return pl.BlockSpec(shape, lambda i: (0,) * len(shape))

    return pl.pallas_call(
        attend_kernel,
        grid=(NC,),
        in_specs=[
            whole(H, TOK, 256),
            whole(ROWS, 960),
            whole(KEYS, 128),
        ]
        + [pl.BlockSpec((1, 256, 256), lambda i: (i, 0, 0))] * NX,
        out_specs=whole(H, PAD, 128),
        out_shape=jax.ShapeDtypeStruct((H, PAD, 128), jnp.bfloat16),
        scratch_shapes=[pltpu.VMEM((GROUP, KEYS, 256), jnp.bfloat16)],
        compiler_params=pltpu.CompilerParams(
            dimension_semantics=("arbitrary",), vmem_limit_bytes=24 * 1024 * 1024
        ),
        cost_estimate=pl.CostEstimate(
            flops=3_000_000_000, bytes_accessed=4_000_000, transcendentals=2_400_000
        ),
        name="attend",
    )(query, lat, seg, *weights)


def merge_kernel(in_ref, out_ref):
    levels = []
    for j in range(H):
        tail = in_ref[j, TOK:, :].astype(jnp.float32)
        levels.append(tail[0:2] + tail[2:4] + tail[4:6])
    top = levels[0]
    for level in levels[1:]:
        top = jnp.maximum(top, level)
    factors = [jnp.exp2(level - top) for level in levels]
    total = factors[0]
    for factor in factors[1:]:
        total = total + factor
    r128 = lax.broadcasted_iota(jnp.int32, (128, 128), 0)
    c128 = lax.broadcasted_iota(jnp.int32, (128, 128), 1)
    acc = jnp.zeros((TOK, 128), jnp.float32)
    for j in range(H):
        share = factors[j] / total
        upper = jnp.sum(jnp.where(r128 == c128, share[0:1], 0.0), axis=1, keepdims=True)
        lower = jnp.sum(
            jnp.where(r128[:64] == c128[:64], share[1:2], 0.0), axis=1, keepdims=True
        )
        column = jnp.concatenate([upper, lower], axis=0)
        acc = acc + column * in_ref[j, :TOK, :].astype(jnp.float32)
    merged = acc.astype(jnp.bfloat16)
    for j in range(H):
        out_ref[j] = merged


def merge(parts):
    return pl.pallas_call(
        merge_kernel,
        out_shape=jax.ShapeDtypeStruct((H, TOK, 128), jnp.bfloat16),
        compiler_params=pltpu.CompilerParams(vmem_limit_bytes=8 * 1024 * 1024),
        cost_estimate=pl.CostEstimate(flops=1_000_000, bytes_accessed=500_000, transcendentals=3000),
        name="merge",
    )(parts)


def mix_kernel(rows_ref, gain_ref, w_hbm, out_ref, n_ref, w_ref, sem):
    copies = [
        pltpu.make_async_copy(w_hbm.at[z], w_ref.at[:, pl.ds(z * 128, 128)], sem.at[z])
        for z in range(NZ)
    ]
    for copy in copies:
        copy.start()
    for y in range(NP):
        square = jnp.zeros((HALF, 256), jnp.float32)
        for f in range(H):
            piece = rows_ref[y * H + f].astype(jnp.float32)
            square = square + piece * piece
        factor = lax.rsqrt(jnp.sum(square, axis=1, keepdims=True) / 2048.0 + epsilon)
        for f in range(H):
            piece = rows_ref[y * H + f].astype(jnp.float32)
            n_ref[y * HALF : (y + 1) * HALF, f * 256 : (f + 1) * 256] = (
                piece * factor * gain_ref[:, f * 256 : (f + 1) * 256]
            ).astype(jnp.bfloat16)
    dims = (((1,), (1,)), ((), ()))
    totals = [None] * (2 * NC)
    for chunk in range(4):
        for copy in copies[chunk * 4 : (chunk + 1) * 4]:
            copy.wait()
        lanes = slice(chunk * 512, (chunk + 1) * 512)
        for k in range(2 * NC):
            start = k // 2 * 1056 + k % 2 * 352
            part = lax.dot_general(
                n_ref[:, lanes], w_ref[start : start + 352, lanes], dims,
                preferred_element_type=jnp.float32,
            )
            totals[k] = part if totals[k] is None else totals[k] + part
    hidden = [
        (totals[2 * c] / (1.0 + jnp.exp(-totals[2 * c])) * totals[2 * c + 1]).astype(jnp.bfloat16)
        for c in range(NC)
    ]
    for f in range(H):
        lanes = slice(f * 256, (f + 1) * 256)
        part = sum(
            jnp.dot(
                hidden[c], w_ref[c * 1056 + 704 : (c + 1) * 1056, lanes],
                preferred_element_type=jnp.float32,
            )
            for c in range(NC)
        ).astype(jnp.bfloat16)
        for y in range(NP):
            out_ref[y * H + f] = part[y * HALF : (y + 1) * HALF]


def mix(rows, gain, weights):
    whole = pl.BlockSpec(memory_space=pltpu.VMEM)
    return pl.pallas_call(
        mix_kernel,
        in_specs=[whole, whole, pl.BlockSpec(memory_space=pltpu.HBM)],
        out_specs=whole,
        out_shape=jax.ShapeDtypeStruct((NP * H, HALF, 256), jnp.bfloat16),
        scratch_shapes=[
            pltpu.VMEM((NP * HALF, 2048), jnp.bfloat16),
            pltpu.VMEM((NC * 1056, 2048), jnp.bfloat16),
            pltpu.SemaphoreType.DMA((NZ,)),
        ],
        compiler_params=pltpu.CompilerParams(vmem_limit_bytes=52_000_000),
        cost_estimate=pl.CostEstimate(
            flops=1_700_000_000, bytes_accessed=10_000_000, transcendentals=140_000
        ),
        name="mix",
    )(rows, gain, weights)


def project_kernel(heads_ref, w_ref, res_ref, mixed_ref, sent_ref):
    heads = jnp.concatenate([heads_ref[h] for h in range(H)], axis=1)
    mixed = (
        res_ref[...].astype(jnp.float32)
        + jnp.dot(heads, w_ref[...], preferred_element_type=jnp.float32)
    ).astype(jnp.bfloat16)
    mixed_ref[...] = mixed
    for d in range(NP * NX):
        for c in range(NC):
            sent_ref[d * NC + c] = mixed[c * HALF : (c + 1) * HALF]


def project(heads, weights, residual):
    return pl.pallas_call(
        project_kernel,
        out_shape=(
            jax.ShapeDtypeStruct((TOK, 256), jnp.bfloat16),
            jax.ShapeDtypeStruct((NP * NX * NC, HALF, 256), jnp.bfloat16),
        ),
        compiler_params=pltpu.CompilerParams(vmem_limit_bytes=12 * 1024 * 1024),
        cost_estimate=pl.CostEstimate(
            flops=100_000_000, bytes_accessed=3_000_000, transcendentals=0
        ),
        name="project",
    )(heads, weights, residual)


def layer(
    query_content,
    query_rotary,
    latents,
    key_rotary,
    latent_gain,
    key_up,
    value_up,
    out_proj,
    residual,
    mixer_gain,
    gate_proj,
    up_proj,
    down_proj,
):
    zi, yi = lax.axis_index("z"), lax.axis_index("g") * NP + lax.axis_index("p")
    sp_index = zi * NY + yi
    tp_index = lax.axis_index("x") * NC + lax.axis_index("c")

    block, inside = tables(np.arange(NZ * NY) * TOK), tables(np.arange(TOK))
    own, kv, cut = prepare(
        latents, key_rotary, latent_gain.reshape(1, -1), block, inside, key_up, value_up,
        gate_proj, up_proj, down_proj.T,
    )
    cut = lax.all_to_all(cut, ("g", "p"), split_axis=0, concat_axis=0, tiled=True)
    mixer = lax.all_gather(put(cut), ("z", "c"), axis=0, tiled=True)
    mixer = mixer.reshape(NZ, NC * 1056, 128)

    lat = lax.all_to_all(own, "z", split_axis=0, concat_axis=0, tiled=True)
    lat = lat.reshape(NZ * 8, 960)
    partner = lax.ppermute(kv, "c", [(0, 1), (1, 0)])
    pair = jnp.stack([kv, partner])
    weights = [pair] + [
        lax.ppermute(pair, "x", [(i, (i + s) % NX) for i in range(NX)]) for s in range(1, NX)
    ]

    lat = lax.all_gather(lat, ("g", "p"), axis=0, tiled=True)

    index = jnp.arange(KEYS, dtype=jnp.int32)
    y_of, z_of, i_of = index // 128 % NY, index // 8 % NZ, index // 512 * 8 + index % 8
    key_segment = (((z_of * NY + y_of) * 8 + tp_index) * 24 + i_of) // SPAN
    ahead_of = (key_segment - sp_index * (TOK // SPAN))[:, None]
    lane = jnp.arange(128, dtype=jnp.int32)[None, :] - DR
    hidden_from = (lane >= 0) & (lane < TOK // SPAN) & (ahead_of > lane)
    seg = jnp.where(hidden_from, masked_score, 0.0).astype(jnp.bfloat16)
    query = turn(query_content, query_rotary, block, inside)
    parts = attend(query, lat, seg, weights)
    parts = lax.all_to_all(parts, ("x", "c"), split_axis=0, concat_axis=0, tiled=True)
    heads = lax.all_to_all(merge(parts), ("x", "c"), split_axis=0, concat_axis=0, tiled=True)
    mixed_rows, sent = project(heads, out_proj, residual)
    rows = lax.all_to_all(sent, ("p", "x", "c"), split_axis=0, concat_axis=0, tiled=True)
    partial_sums = mix(rows, mixer_gain.reshape(1, -1), mixer)
    arrived = lax.all_to_all(
        partial_sums, ("p", "x", "c"), split_axis=0, concat_axis=0, tiled=True
    )
    summed = arrived.reshape(NP * NX, TOK, 256).astype(jnp.float32).sum(axis=0)
    return (mixed_rows.astype(jnp.float32) + summed).astype(jnp.bfloat16)


def solution(mesh):
    fine = Mesh(mesh.devices.reshape(NZ, NY // NP, NP, NX, NC), ("z", "g", "p", "x", "c"))
    sp, tp = ("z", "g", "p"), ("x", "c")
    return jax.shard_map(
        layer,
        mesh=fine,
        in_specs=(
            P(sp, None),
            P(sp, None),
            P((*sp, *tp), None),
            P((*sp, *tp), None),
            P(),
            P(None, tp),
            P(None, tp),
            P(None, tp),
            P(sp, tp),
            P(),
            P(sp, tp),
            P(sp, tp),
            P(tp, sp),
        ),
        out_specs=P(sp, tp),
        check_vma=False,
    )
```

```python
import math

import jax
import jax.numpy as jnp
import numpy as np
from jax import lax
from jax.experimental import pallas as pl
from jax.experimental.pallas import tpu as pltpu
from jax.sharding import Mesh, PartitionSpec as P


H = 8
DN = 128
DR = 64
DV = 128
SPAN = 64
NZ, NY, NX, NC = 16, 4, 4, 2
NP = 2
TOK = 192
HALF = TOK // 2
KEYS = 1536
PAD = 208
ROWS = KEYS // 3

epsilon = 1e-06
masked_score = -1e30
LOG2E = 1.4426950408889634


def tables(places):
    inverse = 10000.0 ** (-np.arange(0, DR, 2) / DR)
    angles = np.tile(places[:, None] * inverse[None, :], (1, 4))
    return jnp.asarray(np.concatenate([np.cos(angles), np.sin(angles)], axis=1), jnp.float32)


def joined(block, inside):
    cos_a, sin_a, cos_b, sin_b = block[:, :128], block[:, 128:], inside[:, :128], inside[:, 128:]
    return cos_a * cos_b - sin_a * sin_b, sin_a * cos_b + cos_a * sin_b


def block_index():
    return lax.axis_index("z") * NY + lax.axis_index("g") * NP + lax.axis_index("p")


def prepare_kernel(
    lat_ref, rot_ref, gain_ref, block_ref, inside_ref, k_ref, v_ref, gate_ref, up_ref, down_ref,
    out_ref, kv_ref, cut_ref,
):
    for k in range(NP):
        block = slice(k * 352, (k + 1) * 352)
        half = jnp.concatenate(
            [gate_ref[:, block], up_ref[:, block], down_ref[:, block]], axis=1
        )
        for y in range(k, NY, NP):
            cut_ref[y] = half
    kv_ref[:, :DN] = k_ref[...]
    kv_ref[:, DN:] = v_ref[...]
    widened = lat_ref[...].astype(jnp.float32)
    factor = lax.rsqrt(jnp.mean(widened * widened, axis=-1, keepdims=True) + epsilon)
    normed = (widened * factor * gain_ref[...]).astype(jnp.bfloat16)
    widened = rot_ref[...].astype(jnp.float32)
    a, b = widened[:, : DR // 2], widened[:, DR // 2 :]
    tp = lax.axis_index("x") * NC + lax.axis_index("c")
    cosine, sine = joined(
        block_ref[pl.ds(block_index(), 1), :],
        inside_ref[pl.ds(pl.multiple_of(tp * 24, 8), 24), :],
    )
    cosine, sine = cosine[:, : DR // 2], sine[:, : DR // 2]
    turned = jnp.concatenate([a * cosine - b * sine, b * cosine + a * sine], axis=-1)
    turned = turned.astype(jnp.bfloat16)
    keys = [slice(j * 8, (j + 1) * 8) for j in range(3)]
    row = jnp.concatenate([normed[k] for k in keys] + [turned[k] for k in keys], axis=1)
    for z in range(NZ):
        out_ref[z] = row


def prepare(*inputs):
    return pl.pallas_call(
        prepare_kernel,
        out_shape=(
            jax.ShapeDtypeStruct((NZ, 8, 960), jnp.bfloat16),
            jax.ShapeDtypeStruct((256, 256), jnp.bfloat16),
            jax.ShapeDtypeStruct((NY, 32, 1056), jnp.bfloat16),
        ),
        compiler_params=pltpu.CompilerParams(vmem_limit_bytes=66_900_000),
        cost_estimate=pl.CostEstimate(flops=100_000, bytes_accessed=300_000, transcendentals=24),
        name="prepare",
    )(*inputs)


def put_kernel(in_ref, out_ref, all_ref):
    for r in range(NY):
        all_ref[r, :, :1056] = in_ref[r].astype(jnp.float32)
    for k in range(9):
        lanes = jnp.concatenate(
            [all_ref[r, :, k * 128 : (k + 1) * 128] for r in range(NY)], axis=0
        )
        rows = min(128, 1056 - k * 128)
        out_ref[k * 128 : k * 128 + rows] = lanes.T[:rows].astype(jnp.bfloat16)


def put(pieces):
    return pl.pallas_call(
        put_kernel,
        out_shape=jax.ShapeDtypeStruct((1056, 128), jnp.bfloat16),
        scratch_shapes=[pltpu.VMEM((NY, 32, 1152), jnp.float32)],
        compiler_params=pltpu.CompilerParams(vmem_limit_bytes=6 * 1024 * 1024),
        cost_estimate=pl.CostEstimate(flops=100_000, bytes_accessed=600_000, transcendentals=0),
        name="put",
    )(pieces)


def turn_kernel(q_ref, qr_ref, block_ref, inside_ref, out_ref):
    cosine, sine = joined(block_ref[pl.ds(block_index(), 1), :], inside_ref[...])
    lane = lax.broadcasted_iota(jnp.int32, (TOK, 2 * DR), 1)
    first = lane % DR < DR // 2
    row = lax.broadcasted_iota(jnp.int32, (TOK, 64), 0)
    col = lax.broadcasted_iota(jnp.int32, (TOK, 64), 1)
    segment = jnp.where(row // SPAN == col, 1.0, 0.0).astype(jnp.bfloat16)
    for pair in range(H // 2):
        turned = qr_ref[:, pair * 2 * DR : (pair + 1) * 2 * DR].astype(jnp.float32)
        swapped = jnp.where(
            first, pltpu.roll(turned, 2 * DR - DR // 2, 1), pltpu.roll(turned, DR // 2, 1)
        )
        signed = jnp.where(first, -swapped, swapped)
        turned = (turned * cosine + signed * sine).astype(jnp.bfloat16)
        for k in range(2):
            h = pair * 2 + k
            out_ref[h, :, :DN] = q_ref[:, h * DN : (h + 1) * DN]
            out_ref[h, :, DN:] = jnp.concatenate(
                [turned[:, k * DR : (k + 1) * DR], segment], axis=1
            )


def turn(*inputs):
    return pl.pallas_call(
        turn_kernel,
        out_shape=jax.ShapeDtypeStruct((H, TOK, 256), jnp.bfloat16),
        compiler_params=pltpu.CompilerParams(vmem_limit_bytes=8 * 1024 * 1024),
        cost_estimate=pl.CostEstimate(flops=500_000, bytes_accessed=1_500_000, transcendentals=0),
        name="turn",
    )(*inputs)


def attend_kernel(q_ref, lat_ref, seg_ref, w0, w1, w2, w3, out_ref, key_ref):
    scale = LOG2E / math.sqrt(DN + DR)
    low = lax.broadcasted_iota(jnp.int32, (ROWS, 128), 1) < DR
    for j in range(3):
        rows = slice(j * ROWS, (j + 1) * ROWS)
        pair = lat_ref[:, 768 + j * DR : 832 + j * DR]
        tail = jnp.where(low, jnp.concatenate([pair, pair], axis=1), seg_ref[rows])
        for h in range(H):
            key_ref[h, rows, DN:] = tail

    ones = jnp.ones((KEYS, 128), jnp.bfloat16)
    r128 = lax.broadcasted_iota(jnp.int32, (128, 128), 0)
    c128 = lax.broadcasted_iota(jnp.int32, (128, 128), 1)

    def scored(turn_at):
        chip = (lax.axis_index("x") + NX - turn_at // NC) % NX
        head = chip * NC + (lax.axis_index("c") + turn_at) % NC
        w_ref = (w0, w1, w2, w3)[turn_at // NC]
        pair = jnp.concatenate(
            [
                jnp.dot(
                    lat_ref[:, j * 256 : (j + 1) * 256], w_ref[turn_at % NC],
                    preferred_element_type=jnp.float32,
                ).astype(jnp.bfloat16)
                for j in range(3)
            ],
            axis=0,
        )
        key_ref[turn_at, :, :DN] = pair[:, :DN]
        scores = lax.dot_general(
            q_ref[head], key_ref[turn_at], (((1,), (1,)), ((), ())),
            preferred_element_type=jnp.float32,
        )
        return head, pair[:, DN:], scores

    following = scored(0)
    for turn_at in range(H):
        head, values, scores = following
        if turn_at + 1 < H:
            following = scored(turn_at + 1)
        highest = jnp.max(scores, axis=1, keepdims=True) * scale
        weights = jnp.exp2(scores * scale - highest).astype(jnp.bfloat16)
        both = jnp.concatenate([values, ones], axis=1)
        sums = jnp.dot(weights, both, preferred_element_type=jnp.float32)
        norm = sums[:, DV:]
        out_ref[head, :TOK, :] = (sums[:, :DV] / norm).astype(jnp.bfloat16)
        level = highest + jnp.log2(norm)
        upper = jnp.sum(jnp.where(r128 == c128, level[:128], 0.0), axis=0, keepdims=True)
        lower = jnp.sum(
            jnp.where(r128[:64] == c128[:64], level[128:], 0.0), axis=0, keepdims=True
        )
        rest = jnp.concatenate([upper, lower], axis=0)
        rows = []
        for _ in range(3):
            part = rest.astype(jnp.bfloat16).astype(jnp.float32)
            rows.append(part)
            rest = rest - part
        rows.append(jnp.zeros((PAD - TOK - 6, 128), jnp.float32))
        out_ref[head, TOK:, :] = jnp.concatenate(rows, axis=0).astype(jnp.bfloat16)


def attend(query, lat, seg, weights):
    return pl.pallas_call(
        attend_kernel,
        out_shape=jax.ShapeDtypeStruct((H, PAD, 128), jnp.bfloat16),
        scratch_shapes=[pltpu.VMEM((H, KEYS, 256), jnp.bfloat16)],
        compiler_params=pltpu.CompilerParams(vmem_limit_bytes=30 * 1024 * 1024),
        cost_estimate=pl.CostEstimate(
            flops=3_000_000_000, bytes_accessed=4_000_000, transcendentals=2_400_000
        ),
        name="attend",
    )(query, lat, seg, *weights)


def merge_kernel(in_ref, out_ref):
    levels = []
    for j in range(H):
        tail = in_ref[j, TOK:, :].astype(jnp.float32)
        levels.append(tail[0:2] + tail[2:4] + tail[4:6])
    top = levels[0]
    for level in levels[1:]:
        top = jnp.maximum(top, level)
    factors = [jnp.exp2(level - top) for level in levels]
    total = factors[0]
    for factor in factors[1:]:
        total = total + factor
    r128 = lax.broadcasted_iota(jnp.int32, (128, 128), 0)
    c128 = lax.broadcasted_iota(jnp.int32, (128, 128), 1)
    acc = jnp.zeros((TOK, 128), jnp.float32)
    for j in range(H):
        share = factors[j] / total
        upper = jnp.sum(jnp.where(r128 == c128, share[0:1], 0.0), axis=1, keepdims=True)
        lower = jnp.sum(
            jnp.where(r128[:64] == c128[:64], share[1:2], 0.0), axis=1, keepdims=True
        )
        column = jnp.concatenate([upper, lower], axis=0)
        acc = acc + column * in_ref[j, :TOK, :].astype(jnp.float32)
    merged = acc.astype(jnp.bfloat16)
    for j in range(H):
        out_ref[j] = merged


def merge(parts):
    return pl.pallas_call(
        merge_kernel,
        out_shape=jax.ShapeDtypeStruct((H, TOK, 128), jnp.bfloat16),
        compiler_params=pltpu.CompilerParams(vmem_limit_bytes=8 * 1024 * 1024),
        cost_estimate=pl.CostEstimate(flops=1_000_000, bytes_accessed=500_000, transcendentals=3000),
        name="merge",
    )(parts)


def mix_kernel(rows_ref, gain_ref, w_hbm, out_ref, n_ref, w_ref, sem):
    copies = [
        pltpu.make_async_copy(w_hbm.at[z], w_ref.at[:, pl.ds(z * 128, 128)], sem.at[z])
        for z in range(NZ)
    ]
    for copy in copies:
        copy.start()
    for y in range(NP):
        square = jnp.zeros((HALF, 256), jnp.float32)
        for f in range(H):
            piece = rows_ref[y * H + f].astype(jnp.float32)
            square = square + piece * piece
        factor = lax.rsqrt(jnp.sum(square, axis=1, keepdims=True) / 2048.0 + epsilon)
        for f in range(H):
            piece = rows_ref[y * H + f].astype(jnp.float32)
            n_ref[y * HALF : (y + 1) * HALF, f * 256 : (f + 1) * 256] = (
                piece * factor * gain_ref[:, f * 256 : (f + 1) * 256]
            ).astype(jnp.bfloat16)
    dims = (((1,), (1,)), ((), ()))
    totals = [None] * (2 * NC)
    for chunk in range(4):
        for copy in copies[chunk * 4 : (chunk + 1) * 4]:
            copy.wait()
        lanes = slice(chunk * 512, (chunk + 1) * 512)
        for k in range(2 * NC):
            start = k // 2 * 1056 + k % 2 * 352
            part = lax.dot_general(
                n_ref[:, lanes], w_ref[start : start + 352, lanes], dims,
                preferred_element_type=jnp.float32,
            )
            totals[k] = part if totals[k] is None else totals[k] + part
    hidden = [
        (totals[2 * c] / (1.0 + jnp.exp(-totals[2 * c])) * totals[2 * c + 1]).astype(jnp.bfloat16)
        for c in range(NC)
    ]
    for f in range(H):
        lanes = slice(f * 256, (f + 1) * 256)
        part = sum(
            jnp.dot(
                hidden[c], w_ref[c * 1056 + 704 : (c + 1) * 1056, lanes],
                preferred_element_type=jnp.float32,
            )
            for c in range(NC)
        ).astype(jnp.bfloat16)
        for y in range(NP):
            out_ref[y * H + f] = part[y * HALF : (y + 1) * HALF]


def mix(rows, gain, weights):
    whole = pl.BlockSpec(memory_space=pltpu.VMEM)
    return pl.pallas_call(
        mix_kernel,
        in_specs=[whole, whole, pl.BlockSpec(memory_space=pltpu.HBM)],
        out_specs=whole,
        out_shape=jax.ShapeDtypeStruct((NP * H, HALF, 256), jnp.bfloat16),
        scratch_shapes=[
            pltpu.VMEM((NP * HALF, 2048), jnp.bfloat16),
            pltpu.VMEM((NC * 1056, 2048), jnp.bfloat16),
            pltpu.SemaphoreType.DMA((NZ,)),
        ],
        compiler_params=pltpu.CompilerParams(vmem_limit_bytes=52_000_000),
        cost_estimate=pl.CostEstimate(
            flops=1_700_000_000, bytes_accessed=10_000_000, transcendentals=140_000
        ),
        name="mix",
    )(rows, gain, weights)


def project_kernel(heads_ref, w_ref, res_ref, mixed_ref, sent_ref):
    heads = jnp.concatenate([heads_ref[h] for h in range(H)], axis=1)
    mixed = (
        res_ref[...].astype(jnp.float32)
        + jnp.dot(heads, w_ref[...], preferred_element_type=jnp.float32)
    ).astype(jnp.bfloat16)
    mixed_ref[...] = mixed
    for d in range(NP * NX):
        for c in range(NC):
            sent_ref[d * NC + c] = mixed[c * HALF : (c + 1) * HALF]


def project(heads, weights, residual):
    return pl.pallas_call(
        project_kernel,
        out_shape=(
            jax.ShapeDtypeStruct((TOK, 256), jnp.bfloat16),
            jax.ShapeDtypeStruct((NP * NX * NC, HALF, 256), jnp.bfloat16),
        ),
        compiler_params=pltpu.CompilerParams(vmem_limit_bytes=12 * 1024 * 1024),
        cost_estimate=pl.CostEstimate(
            flops=100_000_000, bytes_accessed=3_000_000, transcendentals=0
        ),
        name="project",
    )(heads, weights, residual)


def layer(
    query_content,
    query_rotary,
    latents,
    key_rotary,
    latent_gain,
    key_up,
    value_up,
    out_proj,
    residual,
    mixer_gain,
    gate_proj,
    up_proj,
    down_proj,
):
    zi, yi = lax.axis_index("z"), lax.axis_index("g") * NP + lax.axis_index("p")
    sp_index = zi * NY + yi
    tp_index = lax.axis_index("x") * NC + lax.axis_index("c")

    block, inside = tables(np.arange(NZ * NY) * TOK), tables(np.arange(TOK))
    own, kv, cut = prepare(
        latents, key_rotary, latent_gain.reshape(1, -1), block, inside, key_up, value_up,
        gate_proj, up_proj, down_proj.T,
    )
    cut = lax.all_to_all(cut, ("g", "p"), split_axis=0, concat_axis=0, tiled=True)
    mixer = lax.all_gather(put(cut), ("z", "c"), axis=0, tiled=True)
    mixer = mixer.reshape(NZ, NC * 1056, 128)

    lat = lax.all_to_all(own, "z", split_axis=0, concat_axis=0, tiled=True)
    lat = lat.reshape(NZ * 8, 960)
    partner = lax.ppermute(kv, "c", [(0, 1), (1, 0)])
    pair = jnp.stack([kv, partner])
    weights = [pair] + [
        lax.ppermute(pair, "x", [(i, (i + s) % NX) for i in range(NX)]) for s in range(1, NX)
    ]

    lat = lax.all_gather(lat, ("g", "p"), axis=0, tiled=True)

    index = jnp.arange(KEYS, dtype=jnp.int32)
    y_of, z_of, i_of = index // 128 % NY, index // 8 % NZ, index // 512 * 8 + index % 8
    key_segment = (((z_of * NY + y_of) * 8 + tp_index) * 24 + i_of) // SPAN
    ahead_of = (key_segment - sp_index * (TOK // SPAN))[:, None]
    lane = jnp.arange(128, dtype=jnp.int32)[None, :] - DR
    hidden_from = (lane >= 0) & (lane < TOK // SPAN) & (ahead_of > lane)
    seg = jnp.where(hidden_from, masked_score, 0.0).astype(jnp.bfloat16)
    query = turn(query_content, query_rotary, block, inside)
    parts = attend(query, lat, seg, weights)
    parts = lax.all_to_all(parts, ("x", "c"), split_axis=0, concat_axis=0, tiled=True)
    heads = lax.all_to_all(merge(parts), ("x", "c"), split_axis=0, concat_axis=0, tiled=True)
    mixed_rows, sent = project(heads, out_proj, residual)
    rows = lax.all_to_all(sent, ("p", "x", "c"), split_axis=0, concat_axis=0, tiled=True)
    partial_sums = mix(rows, mixer_gain.reshape(1, -1), mixer)
    arrived = lax.all_to_all(
        partial_sums, ("p", "x", "c"), split_axis=0, concat_axis=0, tiled=True
    )
    summed = arrived.reshape(NP * NX, TOK, 256).astype(jnp.float32).sum(axis=0)
    return (mixed_rows.astype(jnp.float32) + summed).astype(jnp.bfloat16)


def solution(mesh):
    fine = Mesh(mesh.devices.reshape(NZ, NY // NP, NP, NX, NC), ("z", "g", "p", "x", "c"))
    sp, tp = ("z", "g", "p"), ("x", "c")
    return jax.shard_map(
        layer,
        mesh=fine,
        in_specs=(
            P(sp, None),
            P(sp, None),
            P((*sp, *tp), None),
            P((*sp, *tp), None),
            P(),
            P(None, tp),
            P(None, tp),
            P(None, tp),
            P(sp, tp),
            P(),
            P(sp, tp),
            P(sp, tp),
            P(tp, sp),
        ),
        out_specs=P(sp, tp),
        check_vma=False,
    )
```

```python
import math

import jax
import jax.numpy as jnp
import numpy as np
from jax import lax
from jax.experimental import pallas as pl
from jax.experimental.pallas import tpu as pltpu
from jax.sharding import Mesh, PartitionSpec as P


H = 8
DN = 128
DR = 64
DV = 128
SPAN = 64
NZ, NY, NX, NC = 16, 4, 4, 2
NP = 2
TOK = 192
HALF = TOK // 2
KEYS = 1536
PAD = 208
ROWS = KEYS // 3

epsilon = 1e-06
masked_score = -1e30
LOG2E = 1.4426950408889634


def tables(places):
    inverse = 10000.0 ** (-np.arange(0, DR, 2) / DR)
    angles = np.tile(places[:, None] * inverse[None, :], (1, 4))
    return jnp.asarray(np.concatenate([np.cos(angles), np.sin(angles)], axis=1), jnp.float32)


def joined(block, inside):
    cos_a, sin_a, cos_b, sin_b = block[:, :128], block[:, 128:], inside[:, :128], inside[:, 128:]
    return cos_a * cos_b - sin_a * sin_b, sin_a * cos_b + cos_a * sin_b


def block_index():
    return lax.axis_index("z") * NY + lax.axis_index("g") * NP + lax.axis_index("p")


def prepare_kernel(
    lat_ref, rot_ref, gain_ref, block_ref, inside_ref, k_ref, v_ref, gate_ref, up_ref, down_ref,
    out_ref, kv_ref, cut_ref,
):
    for k in range(NP):
        block = slice(k * 352, (k + 1) * 352)
        half = jnp.concatenate(
            [gate_ref[:, block], up_ref[:, block], down_ref[:, block]], axis=1
        )
        for y in range(k, NY, NP):
            cut_ref[y] = half
    kv_ref[:, :DN] = k_ref[...]
    kv_ref[:, DN:] = v_ref[...]
    widened = lat_ref[...].astype(jnp.float32)
    factor = lax.rsqrt(jnp.mean(widened * widened, axis=-1, keepdims=True) + epsilon)
    normed = (widened * factor * gain_ref[...]).astype(jnp.bfloat16)
    widened = rot_ref[...].astype(jnp.float32)
    a, b = widened[:, : DR // 2], widened[:, DR // 2 :]
    tp = lax.axis_index("x") * NC + lax.axis_index("c")
    cosine, sine = joined(
        block_ref[pl.ds(block_index(), 1), :],
        inside_ref[pl.ds(pl.multiple_of(tp * 24, 8), 24), :],
    )
    cosine, sine = cosine[:, : DR // 2], sine[:, : DR // 2]
    turned = jnp.concatenate([a * cosine - b * sine, b * cosine + a * sine], axis=-1)
    turned = turned.astype(jnp.bfloat16)
    keys = [slice(j * 8, (j + 1) * 8) for j in range(3)]
    row = jnp.concatenate([normed[k] for k in keys] + [turned[k] for k in keys], axis=1)
    for z in range(NZ):
        out_ref[z] = row


def prepare(*inputs):
    return pl.pallas_call(
        prepare_kernel,
        out_shape=(
            jax.ShapeDtypeStruct((NZ, 8, 960), jnp.bfloat16),
            jax.ShapeDtypeStruct((256, 256), jnp.bfloat16),
            jax.ShapeDtypeStruct((NY, 32, 1056), jnp.bfloat16),
        ),
        compiler_params=pltpu.CompilerParams(vmem_limit_bytes=66_900_000),
        cost_estimate=pl.CostEstimate(flops=100_000, bytes_accessed=300_000, transcendentals=24),
        name="prepare",
    )(*inputs)


def put_kernel(in_ref, out_ref, all_ref):
    for r in range(NY):
        all_ref[r, :, :1056] = in_ref[r].astype(jnp.float32)
    for k in range(9):
        lanes = jnp.concatenate(
            [all_ref[r, :, k * 128 : (k + 1) * 128] for r in range(NY)], axis=0
        )
        rows = min(128, 1056 - k * 128)
        out_ref[k * 128 : k * 128 + rows] = lanes.T[:rows].astype(jnp.bfloat16)


def put(pieces):
    return pl.pallas_call(
        put_kernel,
        out_shape=jax.ShapeDtypeStruct((1056, 128), jnp.bfloat16),
        scratch_shapes=[pltpu.VMEM((NY, 32, 1152), jnp.float32)],
        compiler_params=pltpu.CompilerParams(vmem_limit_bytes=6 * 1024 * 1024),
        cost_estimate=pl.CostEstimate(flops=100_000, bytes_accessed=600_000, transcendentals=0),
        name="put",
    )(pieces)


def turn_kernel(q_ref, qr_ref, block_ref, inside_ref, out_ref):
    cosine, sine = joined(block_ref[pl.ds(block_index(), 1), :], inside_ref[...])
    lane = lax.broadcasted_iota(jnp.int32, (TOK, 2 * DR), 1)
    first = lane % DR < DR // 2
    row = lax.broadcasted_iota(jnp.int32, (TOK, 64), 0)
    col = lax.broadcasted_iota(jnp.int32, (TOK, 64), 1)
    segment = jnp.where(row // SPAN == col, 1.0, 0.0).astype(jnp.bfloat16)
    for pair in range(H // 2):
        turned = qr_ref[:, pair * 2 * DR : (pair + 1) * 2 * DR].astype(jnp.float32)
        swapped = jnp.where(
            first, pltpu.roll(turned, 2 * DR - DR // 2, 1), pltpu.roll(turned, DR // 2, 1)
        )
        signed = jnp.where(first, -swapped, swapped)
        turned = (turned * cosine + signed * sine).astype(jnp.bfloat16)
        for k in range(2):
            h = pair * 2 + k
            out_ref[h, :, :DN] = q_ref[:, h * DN : (h + 1) * DN]
            out_ref[h, :, DN:] = jnp.concatenate(
                [turned[:, k * DR : (k + 1) * DR], segment], axis=1
            )


def turn(*inputs):
    return pl.pallas_call(
        turn_kernel,
        out_shape=jax.ShapeDtypeStruct((H, TOK, 256), jnp.bfloat16),
        compiler_params=pltpu.CompilerParams(vmem_limit_bytes=8 * 1024 * 1024),
        cost_estimate=pl.CostEstimate(flops=500_000, bytes_accessed=1_500_000, transcendentals=0),
        name="turn",
    )(*inputs)


def attend_kernel(q_ref, lat_ref, seg_ref, w0, w1, w2, w3, out_ref, key_ref):
    scale = LOG2E / math.sqrt(DN + DR)
    low = lax.broadcasted_iota(jnp.int32, (ROWS, 128), 1) < DR
    for j in range(3):
        rows = slice(j * ROWS, (j + 1) * ROWS)
        pair = lat_ref[:, 768 + j * DR : 832 + j * DR]
        tail = jnp.where(low, jnp.concatenate([pair, pair], axis=1), seg_ref[rows])
        for h in range(H):
            key_ref[h, rows, DN:] = tail

    ones = jnp.ones((KEYS, 128), jnp.bfloat16)
    r128 = lax.broadcasted_iota(jnp.int32, (128, 128), 0)
    c128 = lax.broadcasted_iota(jnp.int32, (128, 128), 1)

    def scored(turn_at):
        chip = (lax.axis_index("x") + NX - turn_at // NC) % NX
        head = chip * NC + (lax.axis_index("c") + turn_at) % NC
        w_ref = (w0, w1, w2, w3)[turn_at // NC]
        pair = jnp.concatenate(
            [
                jnp.dot(
                    lat_ref[:, j * 256 : (j + 1) * 256], w_ref[turn_at % NC],
                    preferred_element_type=jnp.float32,
                ).astype(jnp.bfloat16)
                for j in range(3)
            ],
            axis=0,
        )
        key_ref[turn_at, :, :DN] = pair[:, :DN]
        scores = lax.dot_general(
            q_ref[head], key_ref[turn_at], (((1,), (1,)), ((), ())),
            preferred_element_type=jnp.float32,
        )
        return head, pair[:, DN:], scores

    following = scored(0)
    for turn_at in range(H):
        head, values, scores = following
        if turn_at + 1 < H:
            following = scored(turn_at + 1)
        highest = jnp.max(scores, axis=1, keepdims=True) * scale
        weights = jnp.exp2(scores * scale - highest).astype(jnp.bfloat16)
        both = jnp.concatenate([values, ones], axis=1)
        sums = jnp.dot(weights, both, preferred_element_type=jnp.float32)
        norm = sums[:, DV:]
        out_ref[head, :TOK, :] = (sums[:, :DV] / norm).astype(jnp.bfloat16)
        level = highest + jnp.log2(norm)
        upper = jnp.sum(jnp.where(r128 == c128, level[:128], 0.0), axis=0, keepdims=True)
        lower = jnp.sum(
            jnp.where(r128[:64] == c128[:64], level[128:], 0.0), axis=0, keepdims=True
        )
        rest = jnp.concatenate([upper, lower], axis=0)
        rows = []
        for _ in range(3):
            part = rest.astype(jnp.bfloat16).astype(jnp.float32)
            rows.append(part)
            rest = rest - part
        rows.append(jnp.zeros((PAD - TOK - 6, 128), jnp.float32))
        out_ref[head, TOK:, :] = jnp.concatenate(rows, axis=0).astype(jnp.bfloat16)


def attend(query, lat, seg, weights):
    return pl.pallas_call(
        attend_kernel,
        out_shape=jax.ShapeDtypeStruct((H, PAD, 128), jnp.bfloat16),
        scratch_shapes=[pltpu.VMEM((H, KEYS, 256), jnp.bfloat16)],
        compiler_params=pltpu.CompilerParams(vmem_limit_bytes=30 * 1024 * 1024),
        cost_estimate=pl.CostEstimate(
            flops=3_000_000_000, bytes_accessed=4_000_000, transcendentals=2_400_000
        ),
        name="attend",
    )(query, lat, seg, *weights)


def merge_kernel(in_ref, out_ref):
    levels = []
    for j in range(H):
        tail = in_ref[j, TOK:, :].astype(jnp.float32)
        levels.append(tail[0:2] + tail[2:4] + tail[4:6])
    top = levels[0]
    for level in levels[1:]:
        top = jnp.maximum(top, level)
    factors = [jnp.exp2(level - top) for level in levels]
    total = factors[0]
    for factor in factors[1:]:
        total = total + factor
    r128 = lax.broadcasted_iota(jnp.int32, (128, 128), 0)
    c128 = lax.broadcasted_iota(jnp.int32, (128, 128), 1)
    acc = jnp.zeros((TOK, 128), jnp.float32)
    for j in range(H):
        share = factors[j] / total
        upper = jnp.sum(jnp.where(r128 == c128, share[0:1], 0.0), axis=1, keepdims=True)
        lower = jnp.sum(
            jnp.where(r128[:64] == c128[:64], share[1:2], 0.0), axis=1, keepdims=True
        )
        column = jnp.concatenate([upper, lower], axis=0)
        acc = acc + column * in_ref[j, :TOK, :].astype(jnp.float32)
    merged = acc.astype(jnp.bfloat16)
    for j in range(H):
        out_ref[j] = merged


def merge(parts):
    return pl.pallas_call(
        merge_kernel,
        out_shape=jax.ShapeDtypeStruct((H, TOK, 128), jnp.bfloat16),
        compiler_params=pltpu.CompilerParams(vmem_limit_bytes=8 * 1024 * 1024),
        cost_estimate=pl.CostEstimate(flops=1_000_000, bytes_accessed=500_000, transcendentals=3000),
        name="merge",
    )(parts)


def mix_kernel(rows_ref, gain_ref, w_hbm, out_ref, n_ref, w_ref, sem):
    def bring(z, c, part, start, rows):
        rows = pl.ds(c * 1056 + start, rows)
        return pltpu.make_async_copy(
            w_hbm.at[z, rows], w_ref.at[rows, pl.ds(z * 128, 128)], sem.at[z, c, part]
        )

    waves = [
        [bring(z, c, 0, 0, 704) for z in range(k * 4, k * 4 + 4) for c in range(NC)]
        for k in range(4)
    ]
    last = [bring(z, c, 1, 704, 352) for z in range(NZ) for c in range(NC)]
    for copy in waves[0] + waves[1]:
        copy.start()
    for y in range(NP):
        square = jnp.zeros((HALF, 256), jnp.float32)
        for f in range(H):
            piece = rows_ref[y * H + f].astype(jnp.float32)
            square = square + piece * piece
        factor = lax.rsqrt(jnp.sum(square, axis=1, keepdims=True) / 2048.0 + epsilon)
        for f in range(H):
            piece = rows_ref[y * H + f].astype(jnp.float32)
            n_ref[y * HALF : (y + 1) * HALF, f * 256 : (f + 1) * 256] = (
                piece * factor * gain_ref[:, f * 256 : (f + 1) * 256]
            ).astype(jnp.bfloat16)
    dims = (((1,), (1,)), ((), ()))
    totals = [None] * (2 * NC)
    for chunk in range(4):
        for copy in waves[chunk]:
            copy.wait()
        for copy in (waves[2], waves[3], last, [])[chunk]:
            copy.start()
        lanes = slice(chunk * 512, (chunk + 1) * 512)
        for k in range(2 * NC):
            start = k // 2 * 1056 + k % 2 * 352
            part = lax.dot_general(
                n_ref[:, lanes], w_ref[start : start + 352, lanes], dims,
                preferred_element_type=jnp.float32,
            )
            totals[k] = part if totals[k] is None else totals[k] + part
    for copy in last:
        copy.wait()
    hidden = [
        (totals[2 * c] / (1.0 + jnp.exp(-totals[2 * c])) * totals[2 * c + 1]).astype(jnp.bfloat16)
        for c in range(NC)
    ]
    for f in range(H):
        lanes = slice(f * 256, (f + 1) * 256)
        part = sum(
            jnp.dot(
                hidden[c], w_ref[c * 1056 + 704 : (c + 1) * 1056, lanes],
                preferred_element_type=jnp.float32,
            )
            for c in range(NC)
        ).astype(jnp.bfloat16)
        for y in range(NP):
            out_ref[y * H + f] = part[y * HALF : (y + 1) * HALF]


def mix(rows, gain, weights):
    whole = pl.BlockSpec(memory_space=pltpu.VMEM)
    return pl.pallas_call(
        mix_kernel,
        in_specs=[whole, whole, pl.BlockSpec(memory_space=pltpu.HBM)],
        out_specs=whole,
        out_shape=jax.ShapeDtypeStruct((NP * H, HALF, 256), jnp.bfloat16),
        scratch_shapes=[
            pltpu.VMEM((NP * HALF, 2048), jnp.bfloat16),
            pltpu.VMEM((NC * 1056, 2048), jnp.bfloat16),
            pltpu.SemaphoreType.DMA((NZ, NC, 2)),
        ],
        compiler_params=pltpu.CompilerParams(vmem_limit_bytes=52_000_000),
        cost_estimate=pl.CostEstimate(
            flops=1_700_000_000, bytes_accessed=10_000_000, transcendentals=140_000
        ),
        name="mix",
    )(rows, gain, weights)


def project_kernel(heads_ref, w_ref, res_ref, mixed_ref, sent_ref):
    heads = jnp.concatenate([heads_ref[h] for h in range(H)], axis=1)
    mixed = (
        res_ref[...].astype(jnp.float32)
        + jnp.dot(heads, w_ref[...], preferred_element_type=jnp.float32)
    ).astype(jnp.bfloat16)
    mixed_ref[...] = mixed
    for d in range(NP * NX):
        for c in range(NC):
            sent_ref[d * NC + c] = mixed[c * HALF : (c + 1) * HALF]


def project(heads, weights, residual):
    return pl.pallas_call(
        project_kernel,
        out_shape=(
            jax.ShapeDtypeStruct((TOK, 256), jnp.bfloat16),
            jax.ShapeDtypeStruct((NP * NX * NC, HALF, 256), jnp.bfloat16),
        ),
        compiler_params=pltpu.CompilerParams(vmem_limit_bytes=12 * 1024 * 1024),
        cost_estimate=pl.CostEstimate(
            flops=100_000_000, bytes_accessed=3_000_000, transcendentals=0
        ),
        name="project",
    )(heads, weights, residual)


def layer(
    query_content,
    query_rotary,
    latents,
    key_rotary,
    latent_gain,
    key_up,
    value_up,
    out_proj,
    residual,
    mixer_gain,
    gate_proj,
    up_proj,
    down_proj,
):
    zi, yi = lax.axis_index("z"), lax.axis_index("g") * NP + lax.axis_index("p")
    sp_index = zi * NY + yi
    tp_index = lax.axis_index("x") * NC + lax.axis_index("c")

    block, inside = tables(np.arange(NZ * NY) * TOK), tables(np.arange(TOK))
    own, kv, cut = prepare(
        latents, key_rotary, latent_gain.reshape(1, -1), block, inside, key_up, value_up,
        gate_proj, up_proj, down_proj.T,
    )
    cut = lax.all_to_all(cut, ("g", "p"), split_axis=0, concat_axis=0, tiled=True)
    mixer = lax.all_gather(put(cut), ("z", "c"), axis=0, tiled=True)
    mixer = mixer.reshape(NZ, NC * 1056, 128)

    lat = lax.all_to_all(own, "z", split_axis=0, concat_axis=0, tiled=True)
    lat = lat.reshape(NZ * 8, 960)
    partner = lax.ppermute(kv, "c", [(0, 1), (1, 0)])
    pair = jnp.stack([kv, partner])
    weights = [pair] + [
        lax.ppermute(pair, "x", [(i, (i + s) % NX) for i in range(NX)]) for s in range(1, NX)
    ]

    lat = lax.all_gather(lat, ("g", "p"), axis=0, tiled=True)

    index = jnp.arange(KEYS, dtype=jnp.int32)
    y_of, z_of, i_of = index // 128 % NY, index // 8 % NZ, index // 512 * 8 + index % 8
    key_segment = (((z_of * NY + y_of) * 8 + tp_index) * 24 + i_of) // SPAN
    ahead_of = (key_segment - sp_index * (TOK // SPAN))[:, None]
    lane = jnp.arange(128, dtype=jnp.int32)[None, :] - DR
    hidden_from = (lane >= 0) & (lane < TOK // SPAN) & (ahead_of > lane)
    seg = jnp.where(hidden_from, masked_score, 0.0).astype(jnp.bfloat16)
    query = turn(query_content, query_rotary, block, inside)
    parts = attend(query, lat, seg, weights)
    parts = lax.all_to_all(parts, ("x", "c"), split_axis=0, concat_axis=0, tiled=True)
    heads = lax.all_to_all(merge(parts), ("x", "c"), split_axis=0, concat_axis=0, tiled=True)
    mixed_rows, sent = project(heads, out_proj, residual)
    rows = lax.all_to_all(sent, ("p", "x", "c"), split_axis=0, concat_axis=0, tiled=True)
    partial_sums = mix(rows, mixer_gain.reshape(1, -1), mixer)
    arrived = lax.all_to_all(
        partial_sums, ("p", "x", "c"), split_axis=0, concat_axis=0, tiled=True
    )
    summed = arrived.reshape(NP * NX, TOK, 256).astype(jnp.float32).sum(axis=0)
    return (mixed_rows.astype(jnp.float32) + summed).astype(jnp.bfloat16)


def solution(mesh):
    fine = Mesh(mesh.devices.reshape(NZ, NY // NP, NP, NX, NC), ("z", "g", "p", "x", "c"))
    sp, tp = ("z", "g", "p"), ("x", "c")
    return jax.shard_map(
        layer,
        mesh=fine,
        in_specs=(
            P(sp, None),
            P(sp, None),
            P((*sp, *tp), None),
            P((*sp, *tp), None),
            P(),
            P(None, tp),
            P(None, tp),
            P(None, tp),
            P(sp, tp),
            P(),
            P(sp, tp),
            P(sp, tp),
            P(tp, sp),
        ),
        out_specs=P(sp, tp),
        check_vma=False,
    )
```
